32 devices in a mesh: grp: 2 (over y), sp: 4 (over z), dp: 4 (over x, core).
Axes of the slice: x: 2, y: 2, z: 4, core: 2. Of those that a mesh axis runs over, the one named last changes fastest.
Arguments:
- tokens: bfloat16 [8, 512, 2048], P(('grp', 'dp'), 'sp'), parts along dimension 0, may hold values from -6 to 6
- forget_offset: float32 [8, 512], P(('grp', 'dp'), 'sp'), parts along dimension 0, may hold values from -1.2 to 1.2, as said below
- q_weight: bfloat16 [2048, 2048], P(None, 'dp'), may hold values from -0.125 to 0.125
- k_weight: bfloat16 [2048, 512], P(None, 'dp'), may hold values from -0.125 to 0.125
- v_weight: bfloat16 [2048, 512], P(None, 'dp'), may hold values from -0.125 to 0.125
- forget_weight: bfloat16 [2048, 16], replicated, may hold values from -0.125 to 0.125
- forget_bias: float32 [16], replicated, may hold values from 3 to 12
- score_gain: float32 [16], replicated, may hold values from 0.5 to 80
- out_gain: float32 [2048], replicated, may hold values from 0.1 to 1.9
Outputs:
- attended: bfloat16 [8, 512, 2048], P(('grp', 'dp'), 'sp'), parts along dimension 0
The draws below stay inside these ranges and needn't reach their ends.
There are 2 independent parts, one for each index of `grp`. The reference program is written for one: setup_inputs(seed, part) draws one part's arguments, and reference() takes and returns one part's arrays. A program takes and returns all parts, laid end to end along the dimension named above; an argument that names none is the same for every part. Nothing has to cross between parts.
Inputs may be any that keep to these rules, and one draw needn't show every extreme that they name: `forget_offset`: constant over aligned spans of 64 positions.
All inputs are finite; a program needn't handle non-finite values.
Results may differ from the reference program's by a relative error of at most 0.0085.
The reference program's roundings to bfloat16 on the way count: a program that leaves them out, or rounds other values in their place, can miss the bound.
Values may be sent and summed in bfloat16 or wider, within the bound.
A program may use at most 128 MiB of HBM per device.

```python
import jax
import jax.numpy as jnp
from jax import lax

WIDTH = 2048
HEADS = 16
KV_HEADS = 4
HEAD_DIM = 128
SEQ_LEN = 512
SEQS = 4


def draw_forget_offset(key, part):
    spans = (SEQ_LEN + 63) // 64
    levels = jax.random.uniform(key, (SEQS, spans), jnp.float32, -1.2, 1.2)
    return jnp.repeat(levels, 64, axis=1)[:, :SEQ_LEN]


def draw_forget_bias(key, part):
    head_order = jax.random.permutation(jax.random.fold_in(key, 11), HEADS)
    jitter = jax.random.uniform(jax.random.fold_in(key, 12), (HEADS,), jnp.float32, -0.3, 0.3)
    slow_level = jnp.log(2.0 * SEQ_LEN)
    fast_level = jnp.log(40.0)
    return jnp.where(head_order < HEADS // 2, slow_level, fast_level) + jitter


def draw_score_gain(key, part):
    return jnp.exp(jax.random.uniform(jax.random.fold_in(key, 22), (HEADS,), jnp.float32, jnp.log(0.7), jnp.log(2.5)))


def steps_of(stream_key, shape, cuts, smallest, largest):
    def one(position, parts):
        draws = jax.random.uniform(jax.random.fold_in(jax.random.fold_in(stream_key, 6), position), (parts,), jnp.float32, smallest / len(cuts), largest / len(cuts))
        return jnp.repeat(jnp.exp(draws), shape[position] // parts).reshape((-1,) + (1,) * (len(shape) - position - 1))

    loudness = one(*cuts[0])
    for cut in cuts[1:]:
        loudness = loudness * one(*cut)
    return loudness


def centred(own_key, shape, scale, bound, split=(), kind=jnp.bfloat16):
    array = scale * jax.random.normal(own_key, shape, jnp.float32)
    if split:
        array = array * steps_of(own_key, shape, split, -0.22, 0.18)
    return jnp.clip(array, -bound, bound).astype(kind)


def setup_inputs(seed: int = 0, part: int = 0) -> dict:
    key_of = jax.random.split(jax.random.key(seed), 10)
    part_splits = jax.random.split(jax.random.fold_in(key_of[9], part), 10)
    return {
        "tokens": centred(part_splits[0], (SEQS, SEQ_LEN, WIDTH), 1.0, 6.0, ((0, 4), (1, 4))),
        "forget_offset": draw_forget_offset(jax.random.fold_in(jax.random.fold_in(key_of[9], part), 71), part),
        "q_weight": centred(key_of[2], (WIDTH, HEADS * HEAD_DIM), WIDTH ** -0.5, 0.125, ((1, 4),)),
        "k_weight": centred(key_of[3], (WIDTH, KV_HEADS * HEAD_DIM), WIDTH ** -0.5, 0.125, ((1, 4),)),
        "v_weight": centred(key_of[4], (WIDTH, KV_HEADS * HEAD_DIM), WIDTH ** -0.5, 0.125, ((1, 4),)),
        "forget_weight": centred(key_of[5], (WIDTH, HEADS), WIDTH ** -0.5, 0.125),
        "forget_bias": draw_forget_bias(jax.random.fold_in(key_of[9], 71), part),
        "score_gain": draw_score_gain(jax.random.fold_in(key_of[9], 71), part),
        "out_gain": jnp.clip(1.0 + 0.18 * jax.random.normal(key_of[8], (HEADS * HEAD_DIM,), jnp.float32), 0.1, 1.9),
    }


NEG = -1e+30
QK_FLOOR = 0.1
OUT_FLOOR = 0.001

def head_norm(vectors, floor):
    return vectors * lax.rsqrt(lax.optimization_barrier(jnp.mean(vectors * vectors, axis=-1, keepdims=True)) + floor)

def attend_sequence(token_rows, offset_rows, q_weight, k_weight, v_weight, forget_weight, forget_bias, score_gain, out_gain):
    length = token_rows.shape[0]
    head_count = forget_bias.shape[0]
    head_dim = out_gain.shape[0] // head_count
    kv_heads = k_weight.shape[1] // head_dim
    group_size = head_count // kv_heads
    queries = jnp.dot(token_rows, q_weight, preferred_element_type=jnp.float32).astype(jnp.bfloat16)
    keys_proj = jnp.dot(token_rows, k_weight, preferred_element_type=jnp.float32).astype(jnp.bfloat16)
    values_proj = jnp.dot(token_rows, v_weight, preferred_element_type=jnp.float32).astype(jnp.bfloat16)
    forget_input = (jnp.dot(token_rows, forget_weight, preferred_element_type=jnp.float32) + offset_rows[:, None]).astype(jnp.bfloat16)
    log_gate = jax.nn.log_sigmoid(forget_input.astype(jnp.float32) + forget_bias[None, :])
    cumulative = jnp.cumsum(log_gate, axis=0).reshape(length, kv_heads, group_size)
    query_unit = head_norm(queries.astype(jnp.float32).reshape(length, kv_heads, group_size, head_dim), QK_FLOOR).astype(jnp.bfloat16)
    key_unit = head_norm(keys_proj.astype(jnp.float32).reshape(length, kv_heads, head_dim), QK_FLOOR).astype(jnp.bfloat16)
    value_heads = values_proj.reshape(length, kv_heads, head_dim)
    factor = (score_gain * head_dim ** (-0.5)).reshape(kv_heads, group_size)
    out_gains = out_gain.reshape(kv_heads, group_size, head_dim)
    span_rows = 512 if length % 512 == 0 else length
    positions = jnp.arange(length, dtype=jnp.int32)
    key_totals = jnp.transpose(cumulative, (1, 2, 0))

    def one_block(block_index):
        first = (block_index * span_rows).astype(jnp.int32)
        query_block = lax.dynamic_slice_in_dim(query_unit, first, span_rows, 0)
        query_totals = lax.dynamic_slice_in_dim(cumulative, first, span_rows, 0)
        scores = jnp.einsum('qkgd,skd->kgqs', query_block.astype(jnp.float32), key_unit.astype(jnp.float32))
        scores = scores * factor[:, :, None, None] + jnp.transpose(query_totals, (1, 2, 0))[..., None] - key_totals[:, :, None, :]
        allowed = positions[None, :] <= (first + jnp.arange(span_rows, dtype=jnp.int32))[:, None]
        scores = jnp.where(allowed[None, None], scores, NEG)
        row_peak = lax.optimization_barrier(jnp.max(scores, axis=-1, keepdims=True))
        exponent = jnp.exp(scores - row_peak)
        weights = (exponent / lax.optimization_barrier(jnp.sum(exponent, axis=-1, keepdims=True))).astype(jnp.bfloat16)
        mixed = jnp.einsum('kgqs,skd->qkgd', weights.astype(jnp.float32), value_heads.astype(jnp.float32))
        return (head_norm(mixed, OUT_FLOOR) * out_gains).astype(jnp.bfloat16)
    outputs = lax.map(one_block, jnp.arange(length // span_rows, dtype=jnp.int32))
    return outputs.reshape(length, head_count * head_dim)

def reference(tokens, forget_offset, q_weight, k_weight, v_weight, forget_weight, forget_bias, score_gain, out_gain):

    def attend_one(one_pair):
        return attend_sequence(one_pair[0], one_pair[1], q_weight, k_weight, v_weight, forget_weight, forget_bias, score_gain, out_gain)
    return lax.map(attend_one, (tokens, forget_offset))
```

```python
import jax
import jax.numpy as jnp
from jax import lax
from jax.experimental import pallas as pl
from jax.experimental.pallas import tpu as pltpu
from jax.sharding import PartitionSpec as P

NEG = -1e30
QK_FLOOR = 0.1
OUT_FLOOR = 0.001


def head_norm(vectors, floor):
    return vectors * lax.rsqrt(jnp.mean(vectors * vectors, axis=-1, keepdims=True) + floor)


def heads_on_sp(
    tokens,
    forget_offset,
    q_weight,
    k_weight,
    v_weight,
    forget_weight,
    forget_bias,
    score_gain,
    out_gain,
):
    own_rows = tokens[0]
    tok_count = own_rows.shape[0]
    head_count = forget_bias.shape[0]
    head_dim = out_gain.shape[0] // head_count
    kv_heads = k_weight.shape[1] * lax.axis_size("dp") // head_dim
    spread = lax.axis_size("sp")
    local_heads = head_count // spread
    local_kv = max(1, kv_heads // spread)
    group_size = local_heads // local_kv
    everyone = lax.all_gather(tokens, "dp", axis=0, tiled=True)
    seq_count = everyone.shape[0]
    flat_rows = everyone.reshape(seq_count * tok_count, everyone.shape[2])
    query_cols = (
        jnp.dot(flat_rows, q_weight, preferred_element_type=jnp.float32)
        .astype(jnp.bfloat16)
        .reshape(seq_count, tok_count, -1)
    )
    key_cols = (
        jnp.dot(flat_rows, k_weight, preferred_element_type=jnp.float32)
        .astype(jnp.bfloat16)
        .reshape(seq_count, tok_count, -1)
    )
    value_cols = (
        jnp.dot(flat_rows, v_weight, preferred_element_type=jnp.float32)
        .astype(jnp.bfloat16)
        .reshape(seq_count, tok_count, -1)
    )
    query_mine, key_mine, value_mine = (
        lax.all_to_all(query_cols, "dp", split_axis=0, concat_axis=2, tiled=True),
        lax.all_to_all(key_cols, "dp", split_axis=0, concat_axis=2, tiled=True),
        lax.all_to_all(value_cols, "dp", split_axis=0, concat_axis=2, tiled=True),
    )
    queries = query_mine[0]
    keys_proj = key_mine[0]
    values_proj = value_mine[0]
    forget_input = (
        jnp.dot(own_rows, forget_weight, preferred_element_type=jnp.float32)
        + forget_offset[0][:, None]
    ).astype(jnp.bfloat16)
    query_send = queries.reshape(tok_count, spread, local_heads, head_dim)
    forget_send = forget_input.reshape(tok_count, spread, local_heads)
    if kv_heads >= spread:
        key_send = keys_proj.reshape(tok_count, spread, local_kv, head_dim)
        value_send = values_proj.reshape(tok_count, spread, local_kv, head_dim)
    else:
        copies = spread // kv_heads
        key_send = jnp.broadcast_to(
            keys_proj.reshape(tok_count, kv_heads, 1, head_dim),
            (tok_count, kv_heads, copies, head_dim),
        ).reshape(tok_count, spread, 1, head_dim)
        value_send = jnp.broadcast_to(
            values_proj.reshape(tok_count, kv_heads, 1, head_dim),
            (tok_count, kv_heads, copies, head_dim),
        ).reshape(tok_count, spread, 1, head_dim)
    query_head, forget_head, key_head, value_head = (
        lax.all_to_all(query_send, "sp", split_axis=1, concat_axis=0, tiled=True),
        lax.all_to_all(forget_send, "sp", split_axis=1, concat_axis=0, tiled=True),
        lax.all_to_all(key_send, "sp", split_axis=1, concat_axis=0, tiled=True),
        lax.all_to_all(value_send, "sp", split_axis=1, concat_axis=0, tiled=True),
    )
    length = query_head.shape[0]
    first_head = lax.axis_index("sp") * local_heads
    bias_local = lax.dynamic_slice_in_dim(forget_bias, first_head, local_heads, 0)
    gain_local = lax.dynamic_slice_in_dim(score_gain, first_head, local_heads, 0)
    norm_local = lax.dynamic_slice_in_dim(
        out_gain, first_head * head_dim, local_heads * head_dim, 0
    )
    log_gate = jax.nn.log_sigmoid(
        forget_head.reshape(length, local_heads).astype(jnp.float32) + bias_local[None, :]
    )
    cumulative = jnp.cumsum(log_gate, axis=0).reshape(length, local_kv, group_size)
    query_unit = head_norm(query_head.astype(jnp.float32), QK_FLOOR).astype(jnp.bfloat16)
    key_unit = head_norm(
        key_head.reshape(length, local_kv, head_dim).astype(jnp.float32), QK_FLOOR
    ).astype(jnp.bfloat16)
    value_heads = value_head.reshape(length, local_kv, head_dim)
    factor = (gain_local * head_dim ** (-0.5)).reshape(local_kv, group_size)
    out_gains = norm_local.reshape(local_kv, group_size, head_dim)
    key_totals = jnp.transpose(cumulative, (1, 2, 0))
    span_rows = 512
    positions = jnp.arange(length, dtype=jnp.int32)

    def attend_block(block_index):
        first = block_index * span_rows
        query_block = lax.dynamic_slice_in_dim(query_unit, first, span_rows, 0)
        query_totals = lax.dynamic_slice_in_dim(cumulative, first, span_rows, 0)
        scores = jnp.einsum(
            "qkgd,skd->kgqs", query_block, key_unit, preferred_element_type=jnp.float32
        )
        scores = (
            scores * factor[:, :, None, None]
            + jnp.transpose(query_totals, (1, 2, 0))[..., None]
            - key_totals[:, :, None, :]
        )
        allowed = positions[None, :] <= (first + jnp.arange(span_rows, dtype=jnp.int32))[:, None]
        scores = jnp.where(allowed[None, None], scores, NEG)
        row_peak = jnp.max(scores, axis=-1, keepdims=True)
        exponent = jnp.exp(scores - row_peak)
        weights = (exponent / jnp.sum(exponent, axis=-1, keepdims=True)).astype(jnp.bfloat16)
        mixed = jnp.einsum(
            "kgqs,skd->qkgd", weights, value_heads, preferred_element_type=jnp.float32
        )
        return (head_norm(mixed, OUT_FLOOR) * out_gains).astype(jnp.bfloat16)

    outputs = lax.map(attend_block, jnp.arange(length // span_rows, dtype=jnp.int32))
    outputs = outputs.reshape(length, local_heads, head_dim)
    back_rows = lax.all_to_all(outputs, "sp", split_axis=0, concat_axis=1, tiled=True)
    return back_rows.reshape(1, tok_count, head_count * head_dim)


def heads_on_dp(
    tokens,
    forget_offset,
    q_weight,
    k_weight,
    v_weight,
    forget_weight,
    forget_bias,
    score_gain,
    out_gain,
):
    tok_count = tokens.shape[1]
    head_count = forget_bias.shape[0]
    head_dim = out_gain.shape[0] // head_count
    seq_count = lax.axis_size("dp")
    kv = k_weight.shape[1] // head_dim
    heads = q_weight.shape[1] // head_dim
    group = heads // kv
    everyone = lax.all_gather(tokens, "dp", axis=0, tiled=True)
    offsets = lax.all_gather(forget_offset, "dp", axis=0, tiled=True)
    flat = everyone.reshape(seq_count * tok_count, -1)
    first = lax.axis_index("dp") * heads

    def mine(array):
        return lax.dynamic_slice_in_dim(array, first, heads, array.ndim - 1)

    def project(weight):
        return jnp.dot(flat, weight, preferred_element_type=jnp.float32).astype(jnp.bfloat16)

    key_unit = head_norm(
        project(k_weight).astype(jnp.float32).reshape(seq_count, tok_count, kv, head_dim), QK_FLOOR
    ).astype(jnp.bfloat16)
    values = project(v_weight).reshape(seq_count, tok_count, kv, head_dim)
    pair = lax.all_gather(jnp.stack([key_unit, values]), "sp", axis=2, tiled=True)
    forget_input = (
        jnp.dot(flat, mine(forget_weight), preferred_element_type=jnp.float32)
        + offsets.reshape(-1)[:, None]
    ).astype(jnp.bfloat16)
    log_gate = jax.nn.log_sigmoid(forget_input.astype(jnp.float32) + mine(forget_bias)[None, :])
    gates = lax.all_gather(
        log_gate.reshape(seq_count, tok_count, heads), "sp", axis=1, tiled=True
    )
    cumulative = jnp.cumsum(gates, axis=1)
    length = gates.shape[1]
    start = lax.axis_index("sp") * tok_count
    own = lax.dynamic_slice_in_dim(cumulative, start, tok_count, 1)
    query_unit = head_norm(
        project(q_weight).astype(jnp.float32).reshape(seq_count, tok_count, kv, group, head_dim),
        QK_FLOOR,
    ).astype(jnp.bfloat16)
    factor = (mine(score_gain) * head_dim ** (-0.5)).reshape(kv, group)
    scores = jnp.einsum(
        "bqkgd,bskd->bkgqs", query_unit, pair[0], preferred_element_type=jnp.float32
    )
    by_head = jnp.transpose(own.reshape(seq_count, tok_count, kv, group), (0, 2, 3, 1))
    by_key = jnp.transpose(cumulative.reshape(seq_count, length, kv, group), (0, 2, 3, 1))
    scores = (
        scores * factor[None, :, :, None, None] + by_head[..., None] - by_key[..., None, :]
    )
    allowed = jnp.arange(length)[None, :] <= (start + jnp.arange(tok_count))[:, None]
    scores = jnp.where(allowed, scores, NEG)
    exponent = jnp.exp(scores - jnp.max(scores, axis=-1, keepdims=True))
    weights = (exponent / jnp.sum(exponent, axis=-1, keepdims=True)).astype(jnp.bfloat16)
    mixed = jnp.einsum(
        "bkgqs,bskd->bqkgd", weights, pair[1], preferred_element_type=jnp.float32
    )
    gains = lax.dynamic_slice_in_dim(out_gain, first * head_dim, heads * head_dim, 0)
    outputs = (head_norm(mixed, OUT_FLOOR) * gains.reshape(kv, group, head_dim)).astype(
        jnp.bfloat16
    )
    outputs = outputs.reshape(seq_count, tok_count, heads * head_dim)
    return lax.all_to_all(outputs, "dp", split_axis=0, concat_axis=2, tiled=True)


def fused_kernel(
    tok_in,
    off_in,
    qw_in,
    kw_in,
    vw_in,
    fw_in,
    bias_in,
    gain_in,
    norm_in,
    out_ref,
    tok,
    qw,
    kvw,
    q_unit,
    kv,
    gate_send,
    gates,
    sent,
    result,
    load_sem,
    tok_send,
    tok_recv,
    gate_send_sem,
    gate_recv_sem,
    kv_send_sem,
    kv_recv_sem,
    chain_send_sem,
    chain_recv_sem,
    out_send_sem,
    out_recv_sem,
    store_sem,
):
    d = lax.axis_index("dp")
    s = lax.axis_index("sp")
    spread = lax.axis_size("sp")
    rows, width = tok_in.shape
    half = rows // 2
    cols = qw_in.shape[1]
    head_dim = kw_in.shape[1]
    heads = cols // head_dim
    seqs = tok.shape[0]
    chip, core = d // 2, d % 2
    last = s == spread - 1

    def peer(step):
        return ((chip + step // 2) % 2) * 2 + (core + step % 2) % 2

    def remote(src, dst, send, recv, **target):
        return pltpu.make_async_remote_copy(
            src_ref=src,
            dst_ref=dst,
            send_sem=send,
            recv_sem=recv,
            device_id=target,
            device_id_type=pl.DeviceIdType.MESH,
        )

    load_tok = pltpu.make_async_copy(tok_in, tok.at[0], load_sem.at[0])
    load_k = pltpu.make_async_copy(kw_in, kvw.at[:, pl.ds(0, head_dim)], load_sem.at[1])
    load_v = pltpu.make_async_copy(vw_in, kvw.at[:, pl.ds(head_dim, head_dim)], load_sem.at[2])
    load_q = pltpu.make_async_copy(qw_in, qw, load_sem.at[3])
    load_tok.start()
    load_k.start()
    load_v.start()
    load_q.start()

    barrier = pltpu.get_barrier_semaphore()
    for step in range(1, seqs):
        pl.semaphore_signal(
            barrier, inc=1, device_id={"dp": peer(step)}, device_id_type=pl.DeviceIdType.MESH
        )

    @pl.when(s > 0)
    def _():
        pl.semaphore_signal(
            barrier, inc=1, device_id={"sp": s - 1}, device_id_type=pl.DeviceIdType.MESH
        )

    @pl.when(s < spread - 1)
    def _():
        pl.semaphore_signal(
            barrier, inc=1, device_id={"sp": s + 1}, device_id_type=pl.DeviceIdType.MESH
        )

    pl.semaphore_wait(barrier, seqs - 1 + (s + spread - 1) // spread + 1 - (s + 1) // spread)

    load_tok.wait()
    parts = [pl.ds(0, half), pl.ds(half, half)]
    over = [
        remote(tok.at[0, part], tok.at[2, part], tok_send.at[1 + i], tok_recv.at[1 + i], dp=peer(2))
        for i, part in enumerate(parts)
    ]
    beside = remote(tok.at[0], tok.at[1], tok_send.at[0], tok_recv.at[0], dp=peer(1))
    onward = [
        remote(tok.at[2, part], tok.at[3, part], tok_send.at[3 + i], tok_recv.at[3 + i], dp=peer(1))
        for i, part in enumerate(parts)
    ]
    over[0].start()
    beside.start()
    over[1].start()

    def unit(vectors):
        vectors = vectors.astype(jnp.bfloat16).astype(jnp.float32)
        return head_norm(vectors, QK_FLOOR).astype(jnp.bfloat16)

    here = pl.ds(pl.multiple_of(s * rows, rows), rows)

    def kv_copy(slot, block):
        piece = kv.at[slot, :, pl.ds(pl.multiple_of(block * rows, rows), rows)]
        return remote(
            piece, piece, kv_send_sem.at[slot, block], kv_recv_sem.at[slot, block],
            sp=(s + 1) % spread,
        )

    def gate_chain(block):
        piece = gates.at[block]
        return remote(
            piece, piece, chain_send_sem.at[block], chain_recv_sem.at[block], sp=(s + 1) % spread
        )

    def project_kv(slot):
        pair = jnp.dot(tok[slot], kvw[...], preferred_element_type=jnp.float32)
        kv[slot, 0, here] = unit(pair[:, :head_dim])
        kv[slot, 1, here] = pair[:, head_dim:].astype(jnp.bfloat16)

        @pl.when(s < spread - 1)
        def _():
            kv_copy(slot, s).start()

    def project_q(slot):
        queries = jnp.dot(tok[slot], qw[...], preferred_element_type=jnp.float32)
        for h in range(heads):
            q_unit[slot, pl.ds(h * rows, rows)] = unit(
                queries[:, h * head_dim : (h + 1) * head_dim]
            )

    load_k.wait()
    load_v.wait()
    project_kv(0)

    forget_input = (
        lax.dot_general(
            fw_in[...], tok[0], (((1,), (1,)), ((), ())), preferred_element_type=jnp.float32
        )
        + off_in[...]
    ).astype(jnp.bfloat16)
    gate_arg = forget_input.astype(jnp.float32) + bias_in[...]
    log_gate = jnp.minimum(gate_arg, 0.0) - jnp.log1p(jnp.exp(-jnp.abs(gate_arg)))
    before = lax.broadcasted_iota(jnp.int32, (rows, rows), 0)
    after = lax.broadcasted_iota(jnp.int32, (rows, rows), 1)
    running = jnp.dot(
        log_gate,
        (before <= after).astype(jnp.float32),
        preferred_element_type=jnp.float32,
        precision=lax.Precision.HIGHEST,
    )
    gate_send[...] = jnp.zeros_like(gate_send)
    for c in range(seqs):
        gate_send[c, :heads, :] = running[c * heads : (c + 1) * heads]
    gates[s, 0] = gate_send[d]
    gate_out = [
        remote(
            gate_send.at[peer(step)], gates.at[s, step], gate_send_sem.at[step],
            gate_recv_sem.at[step], dp=peer(step),
        )
        for step in range(1, seqs)
    ]
    for copy in gate_out:
        copy.start()

    beside.wait_recv()
    project_kv(1)
    load_q.wait()
    project_q(0)
    project_q(1)
    for copy in gate_out:
        copy.wait_recv()

    @pl.when(s < spread - 1)
    def _():
        gate_chain(s).start()

    def relay(k, slots, with_gates):
        block = s - k
        if with_gates:
            gate_chain(block).wait_recv()

            @pl.when(s < spread - 1)
            def _():
                gate_chain(block).start()

        for slot in slots:
            kv_copy(slot, block).wait_recv()

            @pl.when(s < spread - 1)
            def _():
                kv_copy(slot, block).start()

    def early(k, carry):
        relay(k, (0, 1), True)
        return carry

    def late(k, carry):
        relay(k, (2, 3), False)
        return carry

    lax.fori_loop(1, s + 1, early, 0)

    for i in range(2):
        over[i].wait_recv()
        onward[i].start()
    project_kv(2)
    for i in range(2):
        onward[i].wait_recv()
    project_kv(3)
    project_q(2)
    project_q(3)

    @pl.when(s < spread - 1)
    def _():
        lax.fori_loop(1, s + 1, late, 0)

    mine = pl.ds(pl.multiple_of(d * cols, cols), cols)

    def out_copy(slot):
        return remote(
            sent.at[slot], result.at[:, mine], out_send_sem.at[slot], out_recv_sem.at[slot],
            dp=peer(slot),
        )

    def attend(slot, blocks):
        span = blocks * rows
        prefix = jnp.zeros((gates.shape[2], 1), jnp.float32)
        totals = []
        for b in range(blocks):
            local_sum = gates[b, slot]
            totals.append(local_sum + prefix)
            prefix = prefix + local_sum[:, rows - 1 :]
        by_row = jnp.transpose(totals[-1])
        by_key = jnp.concatenate(totals, axis=1)
        row = lax.broadcasted_iota(jnp.int32, (rows, span), 0) + (span - rows)
        column = lax.broadcasted_iota(jnp.int32, (rows, span), 1)
        allowed = column <= row
        keys = kv[slot, 0, :span]
        values = kv[slot, 1, :span]
        for h in range(heads):
            scores = lax.dot_general(
                q_unit[slot, pl.ds(h * rows, rows)],
                keys,
                (((1,), (1,)), ((), ())),
                preferred_element_type=jnp.float32,
            )
            factor = gain_in[0, d * heads + h] * head_dim ** (-0.5)
            scores = scores * factor + by_row[:, h : h + 1] - by_key[h : h + 1, :]
            scores = jnp.where(allowed, scores, NEG)
            exponent = jnp.exp(scores - jnp.max(scores, axis=-1, keepdims=True))
            scale = 1.0 / jnp.sum(exponent, axis=-1, keepdims=True)
            weights = (exponent * scale).astype(jnp.bfloat16)
            mixed = jnp.dot(weights, values, preferred_element_type=jnp.float32)
            gain = norm_in[:, pl.ds(pl.multiple_of(d * cols + h * head_dim, head_dim), head_dim)]
            sent[slot, :, h * head_dim : (h + 1) * head_dim] = (
                head_norm(mixed, OUT_FLOOR) * gain
            ).astype(jnp.bfloat16)

    def each(slot, carry):
        @pl.when(jnp.logical_and(last, slot >= 2))
        def _():
            def arrive(k, inner):
                kv_copy(slot, s - k).wait_recv()
                return inner

            lax.fori_loop(1, s + 1, arrive, 0)

        for k in range(spread):

            @pl.when(s == k)
            def _():
                attend(slot, k + 1)

        @pl.when(slot > 0)
        def _():
            out_copy(slot).start()

        @pl.when(slot == 0)
        def _():
            result[:, mine] = sent[0]

        return carry

    lax.fori_loop(0, seqs, each, 0)

    def flush(slot, carry):
        out_copy(slot).wait_recv()
        return carry

    lax.fori_loop(1, seqs, flush, 0)
    store = pltpu.make_async_copy(result, out_ref, store_sem.at[0])
    store.start()
    for slot in range(1, seqs):
        out_copy(slot).wait_send()
    for copy in over + [beside] + onward + gate_out:
        copy.wait_send()

    @pl.when(s < spread - 1)
    def _():
        def drain(block, carry):
            gate_chain(block).wait_send()
            for slot in range(seqs):
                kv_copy(slot, block).wait_send()
            return carry

        lax.fori_loop(0, s + 1, drain, 0)

    store.wait()


def fused(
    tokens,
    forget_offset,
    q_weight,
    k_weight,
    v_weight,
    forget_weight,
    forget_bias,
    score_gain,
    out_gain,
):
    rows, width = tokens.shape[1:]
    head_count = forget_bias.shape[0]
    head_dim = out_gain.shape[0] // head_count
    seqs = lax.axis_size("dp")
    spread = lax.axis_size("sp")
    cols = q_weight.shape[1]
    heads = cols // head_dim
    padded = -(-heads // 8) * 8
    anywhere = pl.BlockSpec(memory_space=pl.ANY)
    vmem = pl.BlockSpec(memory_space=pltpu.VMEM)
    dma = pltpu.SemaphoreType.DMA
    out = pl.pallas_call(
        fused_kernel,
        out_shape=jax.ShapeDtypeStruct((rows, seqs * cols), jnp.bfloat16),
        in_specs=[anywhere, vmem, anywhere, anywhere, anywhere, vmem, vmem,
                  pl.BlockSpec(memory_space=pltpu.SMEM), vmem],
        out_specs=anywhere,
        scratch_shapes=[
            pltpu.VMEM((seqs, rows, width), jnp.bfloat16),
            pltpu.VMEM((width, cols), jnp.bfloat16),
            pltpu.VMEM((width, 2 * head_dim), jnp.bfloat16),
            pltpu.VMEM((seqs, heads * rows, head_dim), jnp.bfloat16),
            pltpu.VMEM((seqs, 2, spread * rows, head_dim), jnp.bfloat16),
            pltpu.VMEM((seqs, padded, rows), jnp.float32),
            pltpu.VMEM((spread, seqs, padded, rows), jnp.float32),
            pltpu.VMEM((seqs, rows, cols), jnp.bfloat16),
            pltpu.VMEM((rows, seqs * cols), jnp.bfloat16),
            dma((4,)),
            dma((5,)),
            dma((5,)),
            dma((seqs,)),
            dma((seqs,)),
            dma((seqs, spread)),
            dma((seqs, spread)),
            dma((spread,)),
            dma((spread,)),
            dma((seqs,)),
            dma((seqs,)),
            dma((1,)),
        ],
        compiler_params=pltpu.CompilerParams(collective_id=0, has_side_effects=True),
    )(
        tokens[0],
        forget_offset,
        q_weight,
        k_weight,
        v_weight,
        forget_weight.T,
        forget_bias[:, None],
        score_gain[None, :],
        out_gain[None, :],
    )
    return out[None]


def local(*args):
    tokens, k_weight, forget_bias, out_gain = args[0], args[3], args[6], args[8]
    head_dim = out_gain.shape[0] // forget_bias.shape[0]
    if lax.axis_size("dp") == 4 and k_weight.shape[1] == head_dim and tokens.shape[0] == 1:
        return fused(*args)
    if k_weight.shape[1] % head_dim == 0 and tokens.shape[0] == 1:
        return heads_on_dp(*args)
    return heads_on_sp(*args)


def solution(mesh):
    in_specs = (
        P(("grp", "dp"), "sp", None),
        P(("grp", "dp"), "sp"),
        P(None, "dp"),
        P(None, "dp"),
        P(None, "dp"),
        P(),
        P(),
        P(),
        P(),
    )
    out_specs = P(("grp", "dp"), "sp", None)
    return jax.shard_map(local, mesh=mesh, in_specs=in_specs, out_specs=out_specs, check_vma=False)
```

```python
import jax
import jax.numpy as jnp
from jax import lax
from jax.experimental import pallas as pl
from jax.experimental.pallas import tpu as pltpu
from jax.sharding import PartitionSpec as P

NEG = -1e30
QK_FLOOR = 0.1
OUT_FLOOR = 0.001


def head_norm(vectors, floor):
    return vectors * lax.rsqrt(jnp.mean(vectors * vectors, axis=-1, keepdims=True) + floor)


def heads_on_sp(
    tokens,
    forget_offset,
    q_weight,
    k_weight,
    v_weight,
    forget_weight,
    forget_bias,
    score_gain,
    out_gain,
):
    own_rows = tokens[0]
    tok_count = own_rows.shape[0]
    head_count = forget_bias.shape[0]
    head_dim = out_gain.shape[0] // head_count
    kv_heads = k_weight.shape[1] * lax.axis_size("dp") // head_dim
    spread = lax.axis_size("sp")
    local_heads = head_count // spread
    local_kv = max(1, kv_heads // spread)
    group_size = local_heads // local_kv
    everyone = lax.all_gather(tokens, "dp", axis=0, tiled=True)
    seq_count = everyone.shape[0]
    flat_rows = everyone.reshape(seq_count * tok_count, everyone.shape[2])
    query_cols = (
        jnp.dot(flat_rows, q_weight, preferred_element_type=jnp.float32)
        .astype(jnp.bfloat16)
        .reshape(seq_count, tok_count, -1)
    )
    key_cols = (
        jnp.dot(flat_rows, k_weight, preferred_element_type=jnp.float32)
        .astype(jnp.bfloat16)
        .reshape(seq_count, tok_count, -1)
    )
    value_cols = (
        jnp.dot(flat_rows, v_weight, preferred_element_type=jnp.float32)
        .astype(jnp.bfloat16)
        .reshape(seq_count, tok_count, -1)
    )
    query_mine, key_mine, value_mine = (
        lax.all_to_all(query_cols, "dp", split_axis=0, concat_axis=2, tiled=True),
        lax.all_to_all(key_cols, "dp", split_axis=0, concat_axis=2, tiled=True),
        lax.all_to_all(value_cols, "dp", split_axis=0, concat_axis=2, tiled=True),
    )
    queries = query_mine[0]
    keys_proj = key_mine[0]
    values_proj = value_mine[0]
    forget_input = (
        jnp.dot(own_rows, forget_weight, preferred_element_type=jnp.float32)
        + forget_offset[0][:, None]
    ).astype(jnp.bfloat16)
    query_send = queries.reshape(tok_count, spread, local_heads, head_dim)
    forget_send = forget_input.reshape(tok_count, spread, local_heads)
    if kv_heads >= spread:
        key_send = keys_proj.reshape(tok_count, spread, local_kv, head_dim)
        value_send = values_proj.reshape(tok_count, spread, local_kv, head_dim)
    else:
        copies = spread // kv_heads
        key_send = jnp.broadcast_to(
            keys_proj.reshape(tok_count, kv_heads, 1, head_dim),
            (tok_count, kv_heads, copies, head_dim),
        ).reshape(tok_count, spread, 1, head_dim)
        value_send = jnp.broadcast_to(
            values_proj.reshape(tok_count, kv_heads, 1, head_dim),
            (tok_count, kv_heads, copies, head_dim),
        ).reshape(tok_count, spread, 1, head_dim)
    query_head, forget_head, key_head, value_head = (
        lax.all_to_all(query_send, "sp", split_axis=1, concat_axis=0, tiled=True),
        lax.all_to_all(forget_send, "sp", split_axis=1, concat_axis=0, tiled=True),
        lax.all_to_all(key_send, "sp", split_axis=1, concat_axis=0, tiled=True),
        lax.all_to_all(value_send, "sp", split_axis=1, concat_axis=0, tiled=True),
    )
    length = query_head.shape[0]
    first_head = lax.axis_index("sp") * local_heads
    bias_local = lax.dynamic_slice_in_dim(forget_bias, first_head, local_heads, 0)
    gain_local = lax.dynamic_slice_in_dim(score_gain, first_head, local_heads, 0)
    norm_local = lax.dynamic_slice_in_dim(
        out_gain, first_head * head_dim, local_heads * head_dim, 0
    )
    log_gate = jax.nn.log_sigmoid(
        forget_head.reshape(length, local_heads).astype(jnp.float32) + bias_local[None, :]
    )
    cumulative = jnp.cumsum(log_gate, axis=0).reshape(length, local_kv, group_size)
    query_unit = head_norm(query_head.astype(jnp.float32), QK_FLOOR).astype(jnp.bfloat16)
    key_unit = head_norm(
        key_head.reshape(length, local_kv, head_dim).astype(jnp.float32), QK_FLOOR
    ).astype(jnp.bfloat16)
    value_heads = value_head.reshape(length, local_kv, head_dim)
    factor = (gain_local * head_dim ** (-0.5)).reshape(local_kv, group_size)
    out_gains = norm_local.reshape(local_kv, group_size, head_dim)
    key_totals = jnp.transpose(cumulative, (1, 2, 0))
    span_rows = 512
    positions = jnp.arange(length, dtype=jnp.int32)

    def attend_block(block_index):
        first = block_index * span_rows
        query_block = lax.dynamic_slice_in_dim(query_unit, first, span_rows, 0)
        query_totals = lax.dynamic_slice_in_dim(cumulative, first, span_rows, 0)
        scores = jnp.einsum(
            "qkgd,skd->kgqs", query_block, key_unit, preferred_element_type=jnp.float32
        )
        scores = (
            scores * factor[:, :, None, None]
            + jnp.transpose(query_totals, (1, 2, 0))[..., None]
            - key_totals[:, :, None, :]
        )
        allowed = positions[None, :] <= (first + jnp.arange(span_rows, dtype=jnp.int32))[:, None]
        scores = jnp.where(allowed[None, None], scores, NEG)
        row_peak = jnp.max(scores, axis=-1, keepdims=True)
        exponent = jnp.exp(scores - row_peak)
        weights = (exponent / jnp.sum(exponent, axis=-1, keepdims=True)).astype(jnp.bfloat16)
        mixed = jnp.einsum(
            "kgqs,skd->qkgd", weights, value_heads, preferred_element_type=jnp.float32
        )
        return (head_norm(mixed, OUT_FLOOR) * out_gains).astype(jnp.bfloat16)

    outputs = lax.map(attend_block, jnp.arange(length // span_rows, dtype=jnp.int32))
    outputs = outputs.reshape(length, local_heads, head_dim)
    back_rows = lax.all_to_all(outputs, "sp", split_axis=0, concat_axis=1, tiled=True)
    return back_rows.reshape(1, tok_count, head_count * head_dim)


def heads_on_dp(
    tokens,
    forget_offset,
    q_weight,
    k_weight,
    v_weight,
    forget_weight,
    forget_bias,
    score_gain,
    out_gain,
):
    tok_count = tokens.shape[1]
    head_count = forget_bias.shape[0]
    head_dim = out_gain.shape[0] // head_count
    seq_count = lax.axis_size("dp")
    kv = k_weight.shape[1] // head_dim
    heads = q_weight.shape[1] // head_dim
    group = heads // kv
    everyone = lax.all_gather(tokens, "dp", axis=0, tiled=True)
    offsets = lax.all_gather(forget_offset, "dp", axis=0, tiled=True)
    flat = everyone.reshape(seq_count * tok_count, -1)
    first = lax.axis_index("dp") * heads

    def mine(array):
        return lax.dynamic_slice_in_dim(array, first, heads, array.ndim - 1)

    def project(weight):
        return jnp.dot(flat, weight, preferred_element_type=jnp.float32).astype(jnp.bfloat16)

    key_unit = head_norm(
        project(k_weight).astype(jnp.float32).reshape(seq_count, tok_count, kv, head_dim), QK_FLOOR
    ).astype(jnp.bfloat16)
    values = project(v_weight).reshape(seq_count, tok_count, kv, head_dim)
    pair = lax.all_gather(jnp.stack([key_unit, values]), "sp", axis=2, tiled=True)
    forget_input = (
        jnp.dot(flat, mine(forget_weight), preferred_element_type=jnp.float32)
        + offsets.reshape(-1)[:, None]
    ).astype(jnp.bfloat16)
    log_gate = jax.nn.log_sigmoid(forget_input.astype(jnp.float32) + mine(forget_bias)[None, :])
    gates = lax.all_gather(
        log_gate.reshape(seq_count, tok_count, heads), "sp", axis=1, tiled=True
    )
    cumulative = jnp.cumsum(gates, axis=1)
    length = gates.shape[1]
    start = lax.axis_index("sp") * tok_count
    own = lax.dynamic_slice_in_dim(cumulative, start, tok_count, 1)
    query_unit = head_norm(
        project(q_weight).astype(jnp.float32).reshape(seq_count, tok_count, kv, group, head_dim),
        QK_FLOOR,
    ).astype(jnp.bfloat16)
    factor = (mine(score_gain) * head_dim ** (-0.5)).reshape(kv, group)
    scores = jnp.einsum(
        "bqkgd,bskd->bkgqs", query_unit, pair[0], preferred_element_type=jnp.float32
    )
    by_head = jnp.transpose(own.reshape(seq_count, tok_count, kv, group), (0, 2, 3, 1))
    by_key = jnp.transpose(cumulative.reshape(seq_count, length, kv, group), (0, 2, 3, 1))
    scores = (
        scores * factor[None, :, :, None, None] + by_head[..., None] - by_key[..., None, :]
    )
    allowed = jnp.arange(length)[None, :] <= (start + jnp.arange(tok_count))[:, None]
    scores = jnp.where(allowed, scores, NEG)
    exponent = jnp.exp(scores - jnp.max(scores, axis=-1, keepdims=True))
    weights = (exponent / jnp.sum(exponent, axis=-1, keepdims=True)).astype(jnp.bfloat16)
    mixed = jnp.einsum(
        "bkgqs,bskd->bqkgd", weights, pair[1], preferred_element_type=jnp.float32
    )
    gains = lax.dynamic_slice_in_dim(out_gain, first * head_dim, heads * head_dim, 0)
    outputs = (head_norm(mixed, OUT_FLOOR) * gains.reshape(kv, group, head_dim)).astype(
        jnp.bfloat16
    )
    outputs = outputs.reshape(seq_count, tok_count, heads * head_dim)
    return lax.all_to_all(outputs, "dp", split_axis=0, concat_axis=2, tiled=True)


def fused_kernel(
    tok_in,
    off_in,
    qw_in,
    kw_in,
    vw_in,
    fw_in,
    bias_in,
    gain_in,
    norm_in,
    out_ref,
    tok,
    qw,
    kvw,
    q_unit,
    kv,
    gate_send,
    gates,
    sent,
    result,
    load_sem,
    tok_send,
    tok_recv,
    gate_send_sem,
    gate_recv_sem,
    kv_send_sem,
    kv_recv_sem,
    chain_send_sem,
    chain_recv_sem,
    out_send_sem,
    out_recv_sem,
    store_sem,
):
    d = lax.axis_index("dp")
    s = lax.axis_index("sp")
    spread = lax.axis_size("sp")
    rows, width = tok_in.shape
    half = rows // 2
    cols = qw_in.shape[1]
    head_dim = kw_in.shape[1]
    heads = cols // head_dim
    seqs = tok.shape[0]
    chip, core = d // 2, d % 2
    last = s == spread - 1

    def peer(step):
        return ((chip + step // 2) % 2) * 2 + (core + step % 2) % 2

    def remote(src, dst, send, recv, **target):
        return pltpu.make_async_remote_copy(
            src_ref=src,
            dst_ref=dst,
            send_sem=send,
            recv_sem=recv,
            device_id=target,
            device_id_type=pl.DeviceIdType.MESH,
        )

    load_tok = pltpu.make_async_copy(tok_in, tok.at[0], load_sem.at[0])
    load_k = pltpu.make_async_copy(kw_in, kvw.at[:, pl.ds(0, head_dim)], load_sem.at[1])
    load_v = pltpu.make_async_copy(vw_in, kvw.at[:, pl.ds(head_dim, head_dim)], load_sem.at[2])
    load_q = pltpu.make_async_copy(qw_in, qw, load_sem.at[3])
    load_tok.start()
    load_k.start()
    load_v.start()
    load_q.start()

    barrier = pltpu.get_barrier_semaphore()
    for step in range(1, seqs):
        pl.semaphore_signal(
            barrier, inc=1, device_id={"dp": peer(step)}, device_id_type=pl.DeviceIdType.MESH
        )

    @pl.when(s > 0)
    def _():
        pl.semaphore_signal(
            barrier, inc=1, device_id={"sp": s - 1}, device_id_type=pl.DeviceIdType.MESH
        )

    @pl.when(s < spread - 1)
    def _():
        pl.semaphore_signal(
            barrier, inc=1, device_id={"sp": s + 1}, device_id_type=pl.DeviceIdType.MESH
        )

    pl.semaphore_wait(barrier, seqs - 1 + (s + spread - 1) // spread + 1 - (s + 1) // spread)

    load_tok.wait()
    parts = [pl.ds(0, half), pl.ds(half, half)]
    over = [
        remote(tok.at[0, part], tok.at[2, part], tok_send.at[1 + i], tok_recv.at[1 + i], dp=peer(2))
        for i, part in enumerate(parts)
    ]
    beside = remote(tok.at[0], tok.at[1], tok_send.at[0], tok_recv.at[0], dp=peer(1))
    onward = [
        remote(tok.at[2, part], tok.at[3, part], tok_send.at[3 + i], tok_recv.at[3 + i], dp=peer(1))
        for i, part in enumerate(parts)
    ]
    over[0].start()
    beside.start()
    over[1].start()

    def unit(vectors):
        vectors = vectors.astype(jnp.bfloat16).astype(jnp.float32)
        return head_norm(vectors, QK_FLOOR).astype(jnp.bfloat16)

    here = pl.ds(pl.multiple_of(s * rows, rows), rows)

    def pieces(slot):
        return 1 if slot < 2 else 2

    def stretch(slot, piece, block):
        size = rows // pieces(slot)
        return pl.ds(pl.multiple_of(block * rows + piece * size, size), size)

    def kv_copy(slot, piece, block):
        part = kv.at[slot, :, stretch(slot, piece, block)]
        return remote(
            part, part, kv_send_sem.at[slot, piece, block], kv_recv_sem.at[slot, piece, block],
            sp=(s + 1) % spread,
        )

    def gate_chain(block):
        piece = gates.at[block]
        return remote(
            piece, piece, chain_send_sem.at[block], chain_recv_sem.at[block], sp=(s + 1) % spread
        )

    def project_kv(slot, piece):
        size = rows // pieces(slot)
        pair = jnp.dot(
            tok[slot, piece * size : (piece + 1) * size], kvw[...],
            preferred_element_type=jnp.float32,
        )
        place = stretch(slot, piece, s)
        kv[slot, 0, place] = unit(pair[:, :head_dim])
        kv[slot, 1, place] = pair[:, head_dim:].astype(jnp.bfloat16)

        @pl.when(s < spread - 1)
        def _():
            kv_copy(slot, piece, s).start()

    def project_q(slot):
        queries = jnp.dot(tok[slot], qw[...], preferred_element_type=jnp.float32)
        for h in range(heads):
            q_unit[slot, pl.ds(h * rows, rows)] = unit(
                queries[:, h * head_dim : (h + 1) * head_dim]
            )

    load_k.wait()
    load_v.wait()
    project_kv(0, 0)

    forget_input = (
        lax.dot_general(
            fw_in[...], tok[0], (((1,), (1,)), ((), ())), preferred_element_type=jnp.float32
        )
        + off_in[...]
    ).astype(jnp.bfloat16)
    count = bias_in.shape[1]
    square = (count, count)
    diagonal = lax.broadcasted_iota(jnp.int32, square, 0) == lax.broadcasted_iota(
        jnp.int32, square, 1
    )
    bias = jnp.sum(
        jnp.where(diagonal, jnp.broadcast_to(bias_in[...], square), 0.0), axis=1, keepdims=True
    )
    gate_arg = forget_input.astype(jnp.float32) + bias
    log_gate = jnp.minimum(gate_arg, 0.0) - jnp.log1p(jnp.exp(-jnp.abs(gate_arg)))
    before = lax.broadcasted_iota(jnp.int32, (rows, rows), 0)
    after = lax.broadcasted_iota(jnp.int32, (rows, rows), 1)
    running = jnp.dot(
        log_gate,
        (before <= after).astype(jnp.float32),
        preferred_element_type=jnp.float32,
        precision=lax.Precision.HIGHEST,
    )
    gate_send[...] = jnp.zeros_like(gate_send)
    for c in range(seqs):
        gate_send[c, :heads, :] = running[c * heads : (c + 1) * heads]
    gates[s, 0] = gate_send[d]
    gate_out = [
        remote(
            gate_send.at[peer(step)], gates.at[s, step], gate_send_sem.at[step],
            gate_recv_sem.at[step], dp=peer(step),
        )
        for step in range(1, seqs)
    ]
    for copy in gate_out:
        copy.start()

    beside.wait_recv()
    project_kv(1, 0)
    load_q.wait()
    project_q(0)

    def relay(first, stop, units, with_gates=False):
        @pl.when(s < spread - 1)
        def _():
            def one(k, carry):
                block = s - k
                if with_gates:
                    gate_chain(block).wait_recv()
                    gate_chain(block).start()
                for slot, piece in units:
                    kv_copy(slot, piece, block).wait_recv()
                    kv_copy(slot, piece, block).start()
                return carry

            lax.fori_loop(first, stop, one, 0)

    some = (s + spread - 1) // spread
    relay(1, 1 + some, [(0, 0), (1, 0)])
    over[0].wait_recv()
    onward[0].start()
    project_kv(2, 0)
    for copy in gate_out:
        copy.wait_recv()

    @pl.when(s < spread - 1)
    def _():
        gate_chain(s).start()

    project_q(1)
    onward[0].wait_recv()
    project_kv(3, 0)
    relay(2, s + 1, [(0, 0), (1, 0)])
    relay(1, s + 1, [(2, 0), (3, 0)], True)
    over[1].wait_recv()
    onward[1].start()
    project_kv(2, 1)
    onward[1].wait_recv()
    project_kv(3, 1)
    project_q(2)
    relay(1, 1 + some, [(2, 1), (3, 1)])
    project_q(3)
    relay(2, s + 1, [(2, 1), (3, 1)])

    mine = pl.ds(pl.multiple_of(d * cols, cols), cols)

    def out_copy(slot):
        return remote(
            sent.at[slot], result.at[:, mine], out_send_sem.at[slot], out_recv_sem.at[slot],
            dp=peer(slot),
        )

    def attend(slot, blocks):
        span = blocks * rows
        prefix = jnp.zeros((gates.shape[2], 1), jnp.float32)
        totals = []
        for b in range(blocks):
            local_sum = gates[b, slot]
            totals.append(local_sum + prefix)
            prefix = prefix + local_sum[:, rows - 1 :]
        by_row = jnp.transpose(totals[-1])
        by_key = jnp.concatenate(totals, axis=1)
        row = lax.broadcasted_iota(jnp.int32, (rows, span), 0) + (span - rows)
        column = lax.broadcasted_iota(jnp.int32, (rows, span), 1)
        allowed = column <= row
        keys = kv[slot, 0, :span]
        values = kv[slot, 1, :span]
        for h in range(heads):
            scores = lax.dot_general(
                q_unit[slot, pl.ds(h * rows, rows)],
                keys,
                (((1,), (1,)), ((), ())),
                preferred_element_type=jnp.float32,
            )
            factor = gain_in[0, d * heads + h] * head_dim ** (-0.5)
            scores = scores * factor + by_row[:, h : h + 1] - by_key[h : h + 1, :]
            scores = jnp.where(allowed, scores, NEG)
            exponent = jnp.exp(scores - jnp.max(scores, axis=-1, keepdims=True))
            scale = 1.0 / jnp.sum(exponent, axis=-1, keepdims=True)
            weights = (exponent * scale).astype(jnp.bfloat16)
            mixed = jnp.dot(weights, values, preferred_element_type=jnp.float32)
            gain = norm_in[:, pl.ds(pl.multiple_of(d * cols + h * head_dim, head_dim), head_dim)]
            sent[slot, :, h * head_dim : (h + 1) * head_dim] = (
                head_norm(mixed, OUT_FLOOR) * gain
            ).astype(jnp.bfloat16)

    def each(slot, carry):
        for known in range(seqs):

            @pl.when(jnp.logical_and(last, slot == known))
            def _():
                def arrive(k, inner):
                    if known == 0:
                        gate_chain(s - k).wait_recv()
                    for piece in range(pieces(known)):
                        kv_copy(known, piece, s - k).wait_recv()
                    return inner

                lax.fori_loop(1, s + 1, arrive, 0)

        for k in range(spread):

            @pl.when(s == k)
            def _():
                attend(slot, k + 1)

        @pl.when(slot > 0)
        def _():
            out_copy(slot).start()

        @pl.when(slot == 0)
        def _():
            result[:, mine] = sent[0]

        return carry

    lax.fori_loop(0, seqs, each, 0)

    def flush(slot, carry):
        out_copy(slot).wait_recv()
        return carry

    lax.fori_loop(1, seqs, flush, 0)
    store = pltpu.make_async_copy(result, out_ref, store_sem.at[0])
    store.start()
    for slot in range(1, seqs):
        out_copy(slot).wait_send()
    for copy in over + [beside] + onward + gate_out:
        copy.wait_send()

    @pl.when(s < spread - 1)
    def _():
        def drain(block, carry):
            gate_chain(block).wait_send()
            for slot in range(seqs):
                for piece in range(pieces(slot)):
                    kv_copy(slot, piece, block).wait_send()
            return carry

        lax.fori_loop(0, s + 1, drain, 0)

    store.wait()


def fused(
    tokens,
    forget_offset,
    q_weight,
    k_weight,
    v_weight,
    forget_weight,
    forget_bias,
    score_gain,
    out_gain,
):
    rows, width = tokens.shape[1:]
    head_count = forget_bias.shape[0]
    head_dim = out_gain.shape[0] // head_count
    seqs = lax.axis_size("dp")
    spread = lax.axis_size("sp")
    cols = q_weight.shape[1]
    heads = cols // head_dim
    padded = -(-heads // 8) * 8
    anywhere = pl.BlockSpec(memory_space=pl.ANY)
    vmem = pl.BlockSpec(memory_space=pltpu.VMEM)
    dma = pltpu.SemaphoreType.DMA
    out = pl.pallas_call(
        fused_kernel,
        out_shape=jax.ShapeDtypeStruct((rows, seqs * cols), jnp.bfloat16),
        in_specs=[anywhere, vmem, anywhere, anywhere, anywhere, vmem, vmem,
                  pl.BlockSpec(memory_space=pltpu.SMEM), vmem],
        out_specs=anywhere,
        scratch_shapes=[
            pltpu.VMEM((seqs, rows, width), jnp.bfloat16),
            pltpu.VMEM((width, cols), jnp.bfloat16),
            pltpu.VMEM((width, 2 * head_dim), jnp.bfloat16),
            pltpu.VMEM((seqs, heads * rows, head_dim), jnp.bfloat16),
            pltpu.VMEM((seqs, 2, spread * rows, head_dim), jnp.bfloat16),
            pltpu.VMEM((seqs, padded, rows), jnp.float32),
            pltpu.VMEM((spread, seqs, padded, rows), jnp.float32),
            pltpu.VMEM((seqs, rows, cols), jnp.bfloat16),
            pltpu.VMEM((rows, seqs * cols), jnp.bfloat16),
            dma((4,)),
            dma((5,)),
            dma((5,)),
            dma((seqs,)),
            dma((seqs,)),
            dma((seqs, 2, spread)),
            dma((seqs, 2, spread)),
            dma((spread,)),
            dma((spread,)),
            dma((seqs,)),
            dma((seqs,)),
            dma((1,)),
        ],
        compiler_params=pltpu.CompilerParams(collective_id=0, has_side_effects=True),
    )(
        tokens[0],
        forget_offset,
        q_weight,
        k_weight,
        v_weight,
        forget_weight.T,
        forget_bias[None, :],
        score_gain[None, :],
        out_gain[None, :],
    )
    return out[None]


def local(*args):
    tokens, k_weight, forget_bias, out_gain = args[0], args[3], args[6], args[8]
    head_dim = out_gain.shape[0] // forget_bias.shape[0]
    if lax.axis_size("dp") == 4 and k_weight.shape[1] == head_dim and tokens.shape[0] == 1:
        return fused(*args)
    if k_weight.shape[1] % head_dim == 0 and tokens.shape[0] == 1:
        return heads_on_dp(*args)
    return heads_on_sp(*args)


def solution(mesh):
    in_specs = (
        P(("grp", "dp"), "sp", None),
        P(("grp", "dp"), "sp"),
        P(None, "dp"),
        P(None, "dp"),
        P(None, "dp"),
        P(),
        P(),
        P(),
        P(),
    )
    out_specs = P(("grp", "dp"), "sp", None)
    return jax.shard_map(local, mesh=mesh, in_specs=in_specs, out_specs=out_specs, check_vma=False)
```

```python
import jax
import jax.numpy as jnp
from jax import lax
from jax.experimental import pallas as pl
from jax.experimental.pallas import tpu as pltpu
from jax.sharding import PartitionSpec as P

NEG = -1e30
QK_FLOOR = 0.1
OUT_FLOOR = 0.001
SPLITS = 2


def head_norm(vectors, floor):
    return vectors * lax.rsqrt(jnp.mean(vectors * vectors, axis=-1, keepdims=True) + floor)


def heads_on_sp(
    tokens,
    forget_offset,
    q_weight,
    k_weight,
    v_weight,
    forget_weight,
    forget_bias,
    score_gain,
    out_gain,
):
    own_rows = tokens[0]
    tok_count = own_rows.shape[0]
    head_count = forget_bias.shape[0]
    head_dim = out_gain.shape[0] // head_count
    kv_heads = k_weight.shape[1] * lax.axis_size("dp") // head_dim
    spread = lax.axis_size("sp")
    local_heads = head_count // spread
    local_kv = max(1, kv_heads // spread)
    group_size = local_heads // local_kv
    everyone = lax.all_gather(tokens, "dp", axis=0, tiled=True)
    seq_count = everyone.shape[0]
    flat_rows = everyone.reshape(seq_count * tok_count, everyone.shape[2])
    query_cols = (
        jnp.dot(flat_rows, q_weight, preferred_element_type=jnp.float32)
        .astype(jnp.bfloat16)
        .reshape(seq_count, tok_count, -1)
    )
    key_cols = (
        jnp.dot(flat_rows, k_weight, preferred_element_type=jnp.float32)
        .astype(jnp.bfloat16)
        .reshape(seq_count, tok_count, -1)
    )
    value_cols = (
        jnp.dot(flat_rows, v_weight, preferred_element_type=jnp.float32)
        .astype(jnp.bfloat16)
        .reshape(seq_count, tok_count, -1)
    )
    query_mine, key_mine, value_mine = (
        lax.all_to_all(query_cols, "dp", split_axis=0, concat_axis=2, tiled=True),
        lax.all_to_all(key_cols, "dp", split_axis=0, concat_axis=2, tiled=True),
        lax.all_to_all(value_cols, "dp", split_axis=0, concat_axis=2, tiled=True),
    )
    queries = query_mine[0]
    keys_proj = key_mine[0]
    values_proj = value_mine[0]
    forget_input = (
        jnp.dot(own_rows, forget_weight, preferred_element_type=jnp.float32)
        + forget_offset[0][:, None]
    ).astype(jnp.bfloat16)
    query_send = queries.reshape(tok_count, spread, local_heads, head_dim)
    forget_send = forget_input.reshape(tok_count, spread, local_heads)
    if kv_heads >= spread:
        key_send = keys_proj.reshape(tok_count, spread, local_kv, head_dim)
        value_send = values_proj.reshape(tok_count, spread, local_kv, head_dim)
    else:
        copies = spread // kv_heads
        key_send = jnp.broadcast_to(
            keys_proj.reshape(tok_count, kv_heads, 1, head_dim),
            (tok_count, kv_heads, copies, head_dim),
        ).reshape(tok_count, spread, 1, head_dim)
        value_send = jnp.broadcast_to(
            values_proj.reshape(tok_count, kv_heads, 1, head_dim),
            (tok_count, kv_heads, copies, head_dim),
        ).reshape(tok_count, spread, 1, head_dim)
    query_head, forget_head, key_head, value_head = (
        lax.all_to_all(query_send, "sp", split_axis=1, concat_axis=0, tiled=True),
        lax.all_to_all(forget_send, "sp", split_axis=1, concat_axis=0, tiled=True),
        lax.all_to_all(key_send, "sp", split_axis=1, concat_axis=0, tiled=True),
        lax.all_to_all(value_send, "sp", split_axis=1, concat_axis=0, tiled=True),
    )
    length = query_head.shape[0]
    first_head = lax.axis_index("sp") * local_heads
    bias_local = lax.dynamic_slice_in_dim(forget_bias, first_head, local_heads, 0)
    gain_local = lax.dynamic_slice_in_dim(score_gain, first_head, local_heads, 0)
    norm_local = lax.dynamic_slice_in_dim(
        out_gain, first_head * head_dim, local_heads * head_dim, 0
    )
    log_gate = jax.nn.log_sigmoid(
        forget_head.reshape(length, local_heads).astype(jnp.float32) + bias_local[None, :]
    )
    cumulative = jnp.cumsum(log_gate, axis=0).reshape(length, local_kv, group_size)
    query_unit = head_norm(query_head.astype(jnp.float32), QK_FLOOR).astype(jnp.bfloat16)
    key_unit = head_norm(
        key_head.reshape(length, local_kv, head_dim).astype(jnp.float32), QK_FLOOR
    ).astype(jnp.bfloat16)
    value_heads = value_head.reshape(length, local_kv, head_dim)
    factor = (gain_local * head_dim ** (-0.5)).reshape(local_kv, group_size)
    out_gains = norm_local.reshape(local_kv, group_size, head_dim)
    key_totals = jnp.transpose(cumulative, (1, 2, 0))
    span_rows = 512
    positions = jnp.arange(length, dtype=jnp.int32)

    def attend_block(block_index):
        first = block_index * span_rows
        query_block = lax.dynamic_slice_in_dim(query_unit, first, span_rows, 0)
        query_totals = lax.dynamic_slice_in_dim(cumulative, first, span_rows, 0)
        scores = jnp.einsum(
            "qkgd,skd->kgqs", query_block, key_unit, preferred_element_type=jnp.float32
        )
        scores = (
            scores * factor[:, :, None, None]
            + jnp.transpose(query_totals, (1, 2, 0))[..., None]
            - key_totals[:, :, None, :]
        )
        allowed = positions[None, :] <= (first + jnp.arange(span_rows, dtype=jnp.int32))[:, None]
        scores = jnp.where(allowed[None, None], scores, NEG)
        row_peak = jnp.max(scores, axis=-1, keepdims=True)
        exponent = jnp.exp(scores - row_peak)
        weights = (exponent / jnp.sum(exponent, axis=-1, keepdims=True)).astype(jnp.bfloat16)
        mixed = jnp.einsum(
            "kgqs,skd->qkgd", weights, value_heads, preferred_element_type=jnp.float32
        )
        return (head_norm(mixed, OUT_FLOOR) * out_gains).astype(jnp.bfloat16)

    outputs = lax.map(attend_block, jnp.arange(length // span_rows, dtype=jnp.int32))
    outputs = outputs.reshape(length, local_heads, head_dim)
    back_rows = lax.all_to_all(outputs, "sp", split_axis=0, concat_axis=1, tiled=True)
    return back_rows.reshape(1, tok_count, head_count * head_dim)


def heads_on_dp(
    tokens,
    forget_offset,
    q_weight,
    k_weight,
    v_weight,
    forget_weight,
    forget_bias,
    score_gain,
    out_gain,
):
    tok_count = tokens.shape[1]
    head_count = forget_bias.shape[0]
    head_dim = out_gain.shape[0] // head_count
    seq_count = lax.axis_size("dp")
    kv = k_weight.shape[1] // head_dim
    heads = q_weight.shape[1] // head_dim
    group = heads // kv
    everyone = lax.all_gather(tokens, "dp", axis=0, tiled=True)
    offsets = lax.all_gather(forget_offset, "dp", axis=0, tiled=True)
    flat = everyone.reshape(seq_count * tok_count, -1)
    first = lax.axis_index("dp") * heads

    def mine(array):
        return lax.dynamic_slice_in_dim(array, first, heads, array.ndim - 1)

    def project(weight):
        return jnp.dot(flat, weight, preferred_element_type=jnp.float32).astype(jnp.bfloat16)

    key_unit = head_norm(
        project(k_weight).astype(jnp.float32).reshape(seq_count, tok_count, kv, head_dim), QK_FLOOR
    ).astype(jnp.bfloat16)
    values = project(v_weight).reshape(seq_count, tok_count, kv, head_dim)
    pair = lax.all_gather(jnp.stack([key_unit, values]), "sp", axis=2, tiled=True)
    forget_input = (
        jnp.dot(flat, mine(forget_weight), preferred_element_type=jnp.float32)
        + offsets.reshape(-1)[:, None]
    ).astype(jnp.bfloat16)
    log_gate = jax.nn.log_sigmoid(forget_input.astype(jnp.float32) + mine(forget_bias)[None, :])
    gates = lax.all_gather(
        log_gate.reshape(seq_count, tok_count, heads), "sp", axis=1, tiled=True
    )
    cumulative = jnp.cumsum(gates, axis=1)
    length = gates.shape[1]
    start = lax.axis_index("sp") * tok_count
    own = lax.dynamic_slice_in_dim(cumulative, start, tok_count, 1)
    query_unit = head_norm(
        project(q_weight).astype(jnp.float32).reshape(seq_count, tok_count, kv, group, head_dim),
        QK_FLOOR,
    ).astype(jnp.bfloat16)
    factor = (mine(score_gain) * head_dim ** (-0.5)).reshape(kv, group)
    scores = jnp.einsum(
        "bqkgd,bskd->bkgqs", query_unit, pair[0], preferred_element_type=jnp.float32
    )
    by_head = jnp.transpose(own.reshape(seq_count, tok_count, kv, group), (0, 2, 3, 1))
    by_key = jnp.transpose(cumulative.reshape(seq_count, length, kv, group), (0, 2, 3, 1))
    scores = (
        scores * factor[None, :, :, None, None] + by_head[..., None] - by_key[..., None, :]
    )
    allowed = jnp.arange(length)[None, :] <= (start + jnp.arange(tok_count))[:, None]
    scores = jnp.where(allowed, scores, NEG)
    exponent = jnp.exp(scores - jnp.max(scores, axis=-1, keepdims=True))
    weights = (exponent / jnp.sum(exponent, axis=-1, keepdims=True)).astype(jnp.bfloat16)
    mixed = jnp.einsum(
        "bkgqs,bskd->bqkgd", weights, pair[1], preferred_element_type=jnp.float32
    )
    gains = lax.dynamic_slice_in_dim(out_gain, first * head_dim, heads * head_dim, 0)
    outputs = (head_norm(mixed, OUT_FLOOR) * gains.reshape(kv, group, head_dim)).astype(
        jnp.bfloat16
    )
    outputs = outputs.reshape(seq_count, tok_count, heads * head_dim)
    return lax.all_to_all(outputs, "dp", split_axis=0, concat_axis=2, tiled=True)


def fused_kernel(
    tok_in,
    off_in,
    qw_in,
    kw_in,
    vw_in,
    fw_in,
    bias_in,
    gain_in,
    norm_in,
    out_ref,
    tok,
    qw,
    kvw,
    q_unit,
    kv,
    gate_send,
    gates,
    sent,
    result,
    load_sem,
    tok_send,
    tok_recv,
    gate_send_sem,
    gate_recv_sem,
    kv_send_sem,
    kv_recv_sem,
    chain_send_sem,
    chain_recv_sem,
    out_send_sem,
    out_recv_sem,
    store_sem,
):
    d = lax.axis_index("dp")
    s = lax.axis_index("sp")
    spread = lax.axis_size("sp")
    rows, width = tok_in.shape
    splits = kv_send_sem.shape[1]
    size = rows // splits
    cols = qw_in.shape[1]
    head_dim = kw_in.shape[1]
    heads = cols // head_dim
    seqs = tok.shape[0]
    chip, core = d // 2, d % 2
    last = s == spread - 1

    def peer(step):
        return ((chip + step // 2) % 2) * 2 + (core + step % 2) % 2

    def remote(src, dst, send, recv, **target):
        return pltpu.make_async_remote_copy(
            src_ref=src,
            dst_ref=dst,
            send_sem=send,
            recv_sem=recv,
            device_id=target,
            device_id_type=pl.DeviceIdType.MESH,
        )

    load_tok = pltpu.make_async_copy(tok_in, tok.at[0], load_sem.at[0])
    load_k = pltpu.make_async_copy(kw_in, kvw.at[:, pl.ds(0, head_dim)], load_sem.at[1])
    load_v = pltpu.make_async_copy(vw_in, kvw.at[:, pl.ds(head_dim, head_dim)], load_sem.at[2])
    load_q = pltpu.make_async_copy(qw_in, qw, load_sem.at[3])
    load_tok.start()
    load_k.start()
    load_v.start()
    load_q.start()

    barrier = pltpu.get_barrier_semaphore()
    for step in range(1, seqs):
        pl.semaphore_signal(
            barrier, inc=1, device_id={"dp": peer(step)}, device_id_type=pl.DeviceIdType.MESH
        )

    @pl.when(s > 0)
    def _():
        pl.semaphore_signal(
            barrier, inc=1, device_id={"sp": s - 1}, device_id_type=pl.DeviceIdType.MESH
        )

    @pl.when(s < spread - 1)
    def _():
        pl.semaphore_signal(
            barrier, inc=1, device_id={"sp": s + 1}, device_id_type=pl.DeviceIdType.MESH
        )

    pl.semaphore_wait(barrier, seqs - 1 + (s + spread - 1) // spread + 1 - (s + 1) // spread)

    load_tok.wait()
    parts = [pl.ds(i * size, size) for i in range(splits)]
    over = [
        remote(tok.at[0, part], tok.at[2, part], tok_send.at[1 + i], tok_recv.at[1 + i], dp=peer(2))
        for i, part in enumerate(parts)
    ]
    beside = remote(tok.at[0], tok.at[1], tok_send.at[0], tok_recv.at[0], dp=peer(1))
    onward = [
        remote(tok.at[2, part], tok.at[3, part], tok_send.at[1 + splits + i], tok_recv.at[1 + splits + i], dp=peer(1))
        for i, part in enumerate(parts)
    ]
    over[0].start()
    beside.start()
    for copy in over[1:]:
        copy.start()

    def unit(vectors):
        vectors = vectors.astype(jnp.bfloat16).astype(jnp.float32)
        return head_norm(vectors, QK_FLOOR).astype(jnp.bfloat16)

    here = pl.ds(pl.multiple_of(s * rows, rows), rows)

    def pieces(slot):
        return 1 if slot < 2 else splits

    def stretch(slot, piece, block):
        size = rows // pieces(slot)
        return pl.ds(pl.multiple_of(block * rows + piece * size, size), size)

    def kv_copy(slot, piece, block):
        part = kv.at[slot, :, stretch(slot, piece, block)]
        return remote(
            part, part, kv_send_sem.at[slot, piece, block], kv_recv_sem.at[slot, piece, block],
            sp=(s + 1) % spread,
        )

    def gate_chain(block):
        piece = gates.at[block]
        return remote(
            piece, piece, chain_send_sem.at[block], chain_recv_sem.at[block], sp=(s + 1) % spread
        )

    def project_kv(slot, piece):
        size = rows // pieces(slot)
        pair = jnp.dot(
            tok[slot, piece * size : (piece + 1) * size], kvw[...],
            preferred_element_type=jnp.float32,
        )
        place = stretch(slot, piece, s)
        kv[slot, 0, place] = unit(pair[:, :head_dim])
        kv[slot, 1, place] = pair[:, head_dim:].astype(jnp.bfloat16)

        @pl.when(s < spread - 1)
        def _():
            kv_copy(slot, piece, s).start()

    def project_q(slot):
        queries = jnp.dot(tok[slot], qw[...], preferred_element_type=jnp.float32)
        for h in range(heads):
            q_unit[slot, pl.ds(h * rows, rows)] = unit(
                queries[:, h * head_dim : (h + 1) * head_dim]
            )

    load_k.wait()
    load_v.wait()
    project_kv(0, 0)

    forget_input = (
        lax.dot_general(
            fw_in[...], tok[0], (((1,), (1,)), ((), ())), preferred_element_type=jnp.float32
        )
        + off_in[...]
    ).astype(jnp.bfloat16)
    count = bias_in.shape[1]
    square = (count, count)
    diagonal = lax.broadcasted_iota(jnp.int32, square, 0) == lax.broadcasted_iota(
        jnp.int32, square, 1
    )
    bias = jnp.sum(
        jnp.where(diagonal, jnp.broadcast_to(bias_in[...], square), 0.0), axis=1, keepdims=True
    )
    gate_arg = forget_input.astype(jnp.float32) + bias
    log_gate = jnp.minimum(gate_arg, 0.0) - jnp.log1p(jnp.exp(-jnp.abs(gate_arg)))
    before = lax.broadcasted_iota(jnp.int32, (rows, rows), 0)
    after = lax.broadcasted_iota(jnp.int32, (rows, rows), 1)
    running = jnp.dot(
        log_gate,
        (before <= after).astype(jnp.float32),
        preferred_element_type=jnp.float32,
        precision=lax.Precision.HIGHEST,
    )
    gate_send[...] = jnp.zeros_like(gate_send)
    for c in range(seqs):
        gate_send[c, :heads, :] = running[c * heads : (c + 1) * heads]
    gates[s, 0] = gate_send[d]
    gate_out = [
        remote(
            gate_send.at[peer(step)], gates.at[s, step], gate_send_sem.at[step],
            gate_recv_sem.at[step], dp=peer(step),
        )
        for step in range(1, seqs)
    ]
    for copy in gate_out:
        copy.start()

    beside.wait_recv()
    project_kv(1, 0)
    load_q.wait()
    project_q(0)

    def relay(first, stop, units, with_gates=False):
        @pl.when(s < spread - 1)
        def _():
            def one(k, carry):
                block = s - k
                if with_gates:
                    gate_chain(block).wait_recv()
                    gate_chain(block).start()
                for slot, piece in units:
                    kv_copy(slot, piece, block).wait_recv()
                    kv_copy(slot, piece, block).start()
                return carry

            lax.fori_loop(first, stop, one, 0)

    mine = pl.ds(pl.multiple_of(d * cols, cols), cols)

    def out_copy(slot):
        return remote(
            sent.at[slot], result.at[:, mine], out_send_sem.at[slot], out_recv_sem.at[slot],
            dp=peer(slot),
        )

    def attend(slot, blocks):
        span = blocks * rows
        prefix = jnp.zeros((gates.shape[2], 1), jnp.float32)
        totals = []
        for b in range(blocks):
            local_sum = gates[b, slot]
            totals.append(local_sum + prefix)
            prefix = prefix + local_sum[:, rows - 1 :]
        by_row = jnp.transpose(totals[-1])
        by_key = jnp.concatenate(totals, axis=1)
        row = lax.broadcasted_iota(jnp.int32, (rows, span), 0) + (span - rows)
        column = lax.broadcasted_iota(jnp.int32, (rows, span), 1)
        allowed = column <= row
        keys = kv[slot, 0, :span]
        values = kv[slot, 1, :span]
        for h in range(heads):
            scores = lax.dot_general(
                q_unit[slot, pl.ds(h * rows, rows)],
                keys,
                (((1,), (1,)), ((), ())),
                preferred_element_type=jnp.float32,
            )
            factor = gain_in[0, d * heads + h] * head_dim ** (-0.5)
            scores = scores * factor + by_row[:, h : h + 1] - by_key[h : h + 1, :]
            scores = jnp.where(allowed, scores, NEG)
            exponent = jnp.exp(scores - jnp.max(scores, axis=-1, keepdims=True))
            scale = 1.0 / jnp.sum(exponent, axis=-1, keepdims=True)
            weights = (exponent * scale).astype(jnp.bfloat16)
            mixed = jnp.dot(weights, values, preferred_element_type=jnp.float32)
            gain = norm_in[:, pl.ds(pl.multiple_of(d * cols + h * head_dim, head_dim), head_dim)]
            sent[slot, :, h * head_dim : (h + 1) * head_dim] = (
                head_norm(mixed, OUT_FLOOR) * gain
            ).astype(jnp.bfloat16)

    def finish(first, stop, places):
        def each(slot, carry):
            for known in range(first, stop):
                if spread - 1 in places:

                    @pl.when(jnp.logical_and(last, slot == known))
                    def _():
                        def arrive(k, inner):
                            if known == 0:
                                gate_chain(s - k).wait_recv()
                            for piece in range(pieces(known)):
                                kv_copy(known, piece, s - k).wait_recv()
                            return inner

                        lax.fori_loop(1, s + 1, arrive, 0)

            for k in places:

                @pl.when(s == k)
                def _():
                    attend(slot, k + 1)

                    @pl.when(slot > 0)
                    def _():
                        out_copy(slot).start()

                    @pl.when(slot == 0)
                    def _():
                        result[:, mine] = sent[0]

            return carry

        lax.fori_loop(first, stop, each, 0)

    some = (s + spread - 1) // spread
    relay(1, 1 + some, [(0, 0), (1, 0)])
    for i in range(splits):
        over[i].wait_recv()
        onward[i].start()
        project_kv(2, i)
        if i == 0:
            for copy in gate_out:
                copy.wait_recv()

            @pl.when(s < spread - 1)
            def _():
                gate_chain(s).start()

            project_q(1)
        onward[i].wait_recv()
        project_kv(3, i)
        if i == 0:
            relay(2, s + 1, [(0, 0), (1, 0)])
        if i < splits - 1:
            relay(1, s + 1, [(2, i), (3, i)], i == 0)
        if i == splits - 2:
            finish(0, 2, [spread - 1])
    others = list(range(spread - 1))
    project_q(2)
    relay(1, 1 + some, [(2, splits - 1), (3, splits - 1)])
    project_q(3)
    finish(0, 1, others)
    relay(2, s + 1, [(2, splits - 1), (3, splits - 1)])
    finish(1, 2, others)
    finish(2, seqs, others + [spread - 1])


    def flush(slot, carry):
        out_copy(slot).wait_recv()
        return carry

    lax.fori_loop(1, seqs, flush, 0)
    store = pltpu.make_async_copy(result, out_ref, store_sem.at[0])
    store.start()
    for slot in range(1, seqs):
        out_copy(slot).wait_send()
    for copy in over + [beside] + onward + gate_out:
        copy.wait_send()

    @pl.when(s < spread - 1)
    def _():
        def drain(block, carry):
            gate_chain(block).wait_send()
            for slot in range(seqs):
                for piece in range(pieces(slot)):
                    kv_copy(slot, piece, block).wait_send()
            return carry

        lax.fori_loop(0, s + 1, drain, 0)

    store.wait()


def fused(
    tokens,
    forget_offset,
    q_weight,
    k_weight,
    v_weight,
    forget_weight,
    forget_bias,
    score_gain,
    out_gain,
):
    rows, width = tokens.shape[1:]
    head_count = forget_bias.shape[0]
    head_dim = out_gain.shape[0] // head_count
    seqs = lax.axis_size("dp")
    spread = lax.axis_size("sp")
    cols = q_weight.shape[1]
    heads = cols // head_dim
    padded = -(-heads // 8) * 8
    anywhere = pl.BlockSpec(memory_space=pl.ANY)
    vmem = pl.BlockSpec(memory_space=pltpu.VMEM)
    dma = pltpu.SemaphoreType.DMA
    out = pl.pallas_call(
        fused_kernel,
        out_shape=jax.ShapeDtypeStruct((rows, seqs * cols), jnp.bfloat16),
        in_specs=[anywhere, vmem, anywhere, anywhere, anywhere, vmem, vmem,
                  pl.BlockSpec(memory_space=pltpu.SMEM), vmem],
        out_specs=anywhere,
        scratch_shapes=[
            pltpu.VMEM((seqs, rows, width), jnp.bfloat16),
            pltpu.VMEM((width, cols), jnp.bfloat16),
            pltpu.VMEM((width, 2 * head_dim), jnp.bfloat16),
            pltpu.VMEM((seqs, heads * rows, head_dim), jnp.bfloat16),
            pltpu.VMEM((seqs, 2, spread * rows, head_dim), jnp.bfloat16),
            pltpu.VMEM((seqs, padded, rows), jnp.float32),
            pltpu.VMEM((spread, seqs, padded, rows), jnp.float32),
            pltpu.VMEM((seqs, rows, cols), jnp.bfloat16),
            pltpu.VMEM((rows, seqs * cols), jnp.bfloat16),
            dma((4,)),
            dma((1 + 2 * SPLITS,)),
            dma((1 + 2 * SPLITS,)),
            dma((seqs,)),
            dma((seqs,)),
            dma((seqs, SPLITS, spread)),
            dma((seqs, SPLITS, spread)),
            dma((spread,)),
            dma((spread,)),
            dma((seqs,)),
            dma((seqs,)),
            dma((1,)),
        ],
        compiler_params=pltpu.CompilerParams(collective_id=0, has_side_effects=True),
    )(
        tokens[0],
        forget_offset,
        q_weight,
        k_weight,
        v_weight,
        forget_weight.T,
        forget_bias[None, :],
        score_gain[None, :],
        out_gain[None, :],
    )
    return out[None]


def local(*args):
    tokens, k_weight, forget_bias, out_gain = args[0], args[3], args[6], args[8]
    head_dim = out_gain.shape[0] // forget_bias.shape[0]
    if lax.axis_size("dp") == 4 and k_weight.shape[1] == head_dim and tokens.shape[0] == 1:
        return fused(*args)
    if k_weight.shape[1] % head_dim == 0 and tokens.shape[0] == 1:
        return heads_on_dp(*args)
    return heads_on_sp(*args)


def solution(mesh):
    in_specs = (
        P(("grp", "dp"), "sp", None),
        P(("grp", "dp"), "sp"),
        P(None, "dp"),
        P(None, "dp"),
        P(None, "dp"),
        P(),
        P(),
        P(),
        P(),
    )
    out_specs = P(("grp", "dp"), "sp", None)
    return jax.shard_map(local, mesh=mesh, in_specs=in_specs, out_specs=out_specs, check_vma=False)
```

```python
import jax
import jax.numpy as jnp
from jax import lax
from jax.experimental import pallas as pl
from jax.experimental.pallas import tpu as pltpu
from jax.sharding import PartitionSpec as P

NEG = -1e30
QK_FLOOR = 0.1
OUT_FLOOR = 0.001


def head_norm(vectors, floor):
    return vectors * lax.rsqrt(jnp.mean(vectors * vectors, axis=-1, keepdims=True) + floor)


def heads_on_sp(
    tokens,
    forget_offset,
    q_weight,
    k_weight,
    v_weight,
    forget_weight,
    forget_bias,
    score_gain,
    out_gain,
):
    own_rows = tokens[0]
    tok_count = own_rows.shape[0]
    head_count = forget_bias.shape[0]
    head_dim = out_gain.shape[0] // head_count
    kv_heads = k_weight.shape[1] * lax.axis_size("dp") // head_dim
    spread = lax.axis_size("sp")
    local_heads = head_count // spread
    local_kv = max(1, kv_heads // spread)
    group_size = local_heads // local_kv
    everyone = lax.all_gather(tokens, "dp", axis=0, tiled=True)
    seq_count = everyone.shape[0]
    flat_rows = everyone.reshape(seq_count * tok_count, everyone.shape[2])
    query_cols = (
        jnp.dot(flat_rows, q_weight, preferred_element_type=jnp.float32)
        .astype(jnp.bfloat16)
        .reshape(seq_count, tok_count, -1)
    )
    key_cols = (
        jnp.dot(flat_rows, k_weight, preferred_element_type=jnp.float32)
        .astype(jnp.bfloat16)
        .reshape(seq_count, tok_count, -1)
    )
    value_cols = (
        jnp.dot(flat_rows, v_weight, preferred_element_type=jnp.float32)
        .astype(jnp.bfloat16)
        .reshape(seq_count, tok_count, -1)
    )
    query_mine, key_mine, value_mine = (
        lax.all_to_all(query_cols, "dp", split_axis=0, concat_axis=2, tiled=True),
        lax.all_to_all(key_cols, "dp", split_axis=0, concat_axis=2, tiled=True),
        lax.all_to_all(value_cols, "dp", split_axis=0, concat_axis=2, tiled=True),
    )
    queries = query_mine[0]
    keys_proj = key_mine[0]
    values_proj = value_mine[0]
    forget_input = (
        jnp.dot(own_rows, forget_weight, preferred_element_type=jnp.float32)
        + forget_offset[0][:, None]
    ).astype(jnp.bfloat16)
    query_send = queries.reshape(tok_count, spread, local_heads, head_dim)
    forget_send = forget_input.reshape(tok_count, spread, local_heads)
    if kv_heads >= spread:
        key_send = keys_proj.reshape(tok_count, spread, local_kv, head_dim)
        value_send = values_proj.reshape(tok_count, spread, local_kv, head_dim)
    else:
        copies = spread // kv_heads
        key_send = jnp.broadcast_to(
            keys_proj.reshape(tok_count, kv_heads, 1, head_dim),
            (tok_count, kv_heads, copies, head_dim),
        ).reshape(tok_count, spread, 1, head_dim)
        value_send = jnp.broadcast_to(
            values_proj.reshape(tok_count, kv_heads, 1, head_dim),
            (tok_count, kv_heads, copies, head_dim),
        ).reshape(tok_count, spread, 1, head_dim)
    query_head, forget_head, key_head, value_head = (
        lax.all_to_all(query_send, "sp", split_axis=1, concat_axis=0, tiled=True),
        lax.all_to_all(forget_send, "sp", split_axis=1, concat_axis=0, tiled=True),
        lax.all_to_all(key_send, "sp", split_axis=1, concat_axis=0, tiled=True),
        lax.all_to_all(value_send, "sp", split_axis=1, concat_axis=0, tiled=True),
    )
    length = query_head.shape[0]
    first_head = lax.axis_index("sp") * local_heads
    bias_local = lax.dynamic_slice_in_dim(forget_bias, first_head, local_heads, 0)
    gain_local = lax.dynamic_slice_in_dim(score_gain, first_head, local_heads, 0)
    norm_local = lax.dynamic_slice_in_dim(
        out_gain, first_head * head_dim, local_heads * head_dim, 0
    )
    log_gate = jax.nn.log_sigmoid(
        forget_head.reshape(length, local_heads).astype(jnp.float32) + bias_local[None, :]
    )
    cumulative = jnp.cumsum(log_gate, axis=0).reshape(length, local_kv, group_size)
    query_unit = head_norm(query_head.astype(jnp.float32), QK_FLOOR).astype(jnp.bfloat16)
    key_unit = head_norm(
        key_head.reshape(length, local_kv, head_dim).astype(jnp.float32), QK_FLOOR
    ).astype(jnp.bfloat16)
    value_heads = value_head.reshape(length, local_kv, head_dim)
    factor = (gain_local * head_dim ** (-0.5)).reshape(local_kv, group_size)
    out_gains = norm_local.reshape(local_kv, group_size, head_dim)
    key_totals = jnp.transpose(cumulative, (1, 2, 0))
    span_rows = 512
    positions = jnp.arange(length, dtype=jnp.int32)

    def attend_block(block_index):
        first = block_index * span_rows
        query_block = lax.dynamic_slice_in_dim(query_unit, first, span_rows, 0)
        query_totals = lax.dynamic_slice_in_dim(cumulative, first, span_rows, 0)
        scores = jnp.einsum(
            "qkgd,skd->kgqs", query_block, key_unit, preferred_element_type=jnp.float32
        )
        scores = (
            scores * factor[:, :, None, None]
            + jnp.transpose(query_totals, (1, 2, 0))[..., None]
            - key_totals[:, :, None, :]
        )
        allowed = positions[None, :] <= (first + jnp.arange(span_rows, dtype=jnp.int32))[:, None]
        scores = jnp.where(allowed[None, None], scores, NEG)
        row_peak = jnp.max(scores, axis=-1, keepdims=True)
        exponent = jnp.exp(scores - row_peak)
        weights = (exponent / jnp.sum(exponent, axis=-1, keepdims=True)).astype(jnp.bfloat16)
        mixed = jnp.einsum(
            "kgqs,skd->qkgd", weights, value_heads, preferred_element_type=jnp.float32
        )
        return (head_norm(mixed, OUT_FLOOR) * out_gains).astype(jnp.bfloat16)

    outputs = lax.map(attend_block, jnp.arange(length // span_rows, dtype=jnp.int32))
    outputs = outputs.reshape(length, local_heads, head_dim)
    back_rows = lax.all_to_all(outputs, "sp", split_axis=0, concat_axis=1, tiled=True)
    return back_rows.reshape(1, tok_count, head_count * head_dim)


def heads_on_dp(
    tokens,
    forget_offset,
    q_weight,
    k_weight,
    v_weight,
    forget_weight,
    forget_bias,
    score_gain,
    out_gain,
):
    tok_count = tokens.shape[1]
    head_count = forget_bias.shape[0]
    head_dim = out_gain.shape[0] // head_count
    seq_count = lax.axis_size("dp")
    kv = k_weight.shape[1] // head_dim
    heads = q_weight.shape[1] // head_dim
    group = heads // kv
    everyone = lax.all_gather(tokens, "dp", axis=0, tiled=True)
    offsets = lax.all_gather(forget_offset, "dp", axis=0, tiled=True)
    flat = everyone.reshape(seq_count * tok_count, -1)
    first = lax.axis_index("dp") * heads

    def mine(array):
        return lax.dynamic_slice_in_dim(array, first, heads, array.ndim - 1)

    def project(weight):
        return jnp.dot(flat, weight, preferred_element_type=jnp.float32).astype(jnp.bfloat16)

    key_unit = head_norm(
        project(k_weight).astype(jnp.float32).reshape(seq_count, tok_count, kv, head_dim), QK_FLOOR
    ).astype(jnp.bfloat16)
    values = project(v_weight).reshape(seq_count, tok_count, kv, head_dim)
    pair = lax.all_gather(jnp.stack([key_unit, values]), "sp", axis=2, tiled=True)
    forget_input = (
        jnp.dot(flat, mine(forget_weight), preferred_element_type=jnp.float32)
        + offsets.reshape(-1)[:, None]
    ).astype(jnp.bfloat16)
    log_gate = jax.nn.log_sigmoid(forget_input.astype(jnp.float32) + mine(forget_bias)[None, :])
    gates = lax.all_gather(
        log_gate.reshape(seq_count, tok_count, heads), "sp", axis=1, tiled=True
    )
    cumulative = jnp.cumsum(gates, axis=1)
    length = gates.shape[1]
    start = lax.axis_index("sp") * tok_count
    own = lax.dynamic_slice_in_dim(cumulative, start, tok_count, 1)
    query_unit = head_norm(
        project(q_weight).astype(jnp.float32).reshape(seq_count, tok_count, kv, group, head_dim),
        QK_FLOOR,
    ).astype(jnp.bfloat16)
    factor = (mine(score_gain) * head_dim ** (-0.5)).reshape(kv, group)
    scores = jnp.einsum(
        "bqkgd,bskd->bkgqs", query_unit, pair[0], preferred_element_type=jnp.float32
    )
    by_head = jnp.transpose(own.reshape(seq_count, tok_count, kv, group), (0, 2, 3, 1))
    by_key = jnp.transpose(cumulative.reshape(seq_count, length, kv, group), (0, 2, 3, 1))
    scores = (
        scores * factor[None, :, :, None, None] + by_head[..., None] - by_key[..., None, :]
    )
    allowed = jnp.arange(length)[None, :] <= (start + jnp.arange(tok_count))[:, None]
    scores = jnp.where(allowed, scores, NEG)
    exponent = jnp.exp(scores - jnp.max(scores, axis=-1, keepdims=True))
    weights = (exponent / jnp.sum(exponent, axis=-1, keepdims=True)).astype(jnp.bfloat16)
    mixed = jnp.einsum(
        "bkgqs,bskd->bqkgd", weights, pair[1], preferred_element_type=jnp.float32
    )
    gains = lax.dynamic_slice_in_dim(out_gain, first * head_dim, heads * head_dim, 0)
    outputs = (head_norm(mixed, OUT_FLOOR) * gains.reshape(kv, group, head_dim)).astype(
        jnp.bfloat16
    )
    outputs = outputs.reshape(seq_count, tok_count, heads * head_dim)
    return lax.all_to_all(outputs, "dp", split_axis=0, concat_axis=2, tiled=True)


def fused_kernel(
    tok_in,
    off_in,
    qw_in,
    kw_in,
    vw_in,
    fw_in,
    bias_in,
    gain_in,
    norm_in,
    out_ref,
    tok,
    qw,
    kvw,
    q_unit,
    kv,
    gate_send,
    gates,
    sent,
    result,
    load_sem,
    tok_send,
    tok_recv,
    gate_send_sem,
    gate_recv_sem,
    kv_send_sem,
    kv_recv_sem,
    chain_send_sem,
    chain_recv_sem,
    out_send_sem,
    out_recv_sem,
    store_sem,
):
    d = lax.axis_index("dp")
    s = lax.axis_index("sp")
    spread = lax.axis_size("sp")
    rows, width = tok_in.shape
    half = rows // 2
    cols = qw_in.shape[1]
    head_dim = kw_in.shape[1]
    heads = cols // head_dim
    seqs = tok.shape[0]
    chip, core = d // 2, d % 2
    last = s == spread - 1

    def peer(step):
        across = step // 2
        own_chip = (1 - across) * ((core + step % 2) % 2)
        return ((chip + across) % 2) * 2 + across * (step % 2) + own_chip

    def seen_as(step):
        return (step // 2) * (2 + core) + (1 - step // 2) * step

    def remote(src, dst, send, recv, **target):
        return pltpu.make_async_remote_copy(
            src_ref=src,
            dst_ref=dst,
            send_sem=send,
            recv_sem=recv,
            device_id=target,
            device_id_type=pl.DeviceIdType.MESH,
        )

    load_tok = pltpu.make_async_copy(tok_in, tok.at[0], load_sem.at[0])
    load_k = pltpu.make_async_copy(kw_in, kvw.at[:, pl.ds(0, head_dim)], load_sem.at[1])
    load_v = pltpu.make_async_copy(vw_in, kvw.at[:, pl.ds(head_dim, head_dim)], load_sem.at[2])
    load_q = pltpu.make_async_copy(qw_in, qw, load_sem.at[3])
    load_tok.start()
    load_k.start()
    load_v.start()
    load_q.start()

    barrier = pltpu.get_barrier_semaphore()
    for step in range(1, seqs):
        pl.semaphore_signal(
            barrier, inc=1, device_id={"dp": peer(step)}, device_id_type=pl.DeviceIdType.MESH
        )

    @pl.when(s > 0)
    def _():
        pl.semaphore_signal(
            barrier, inc=1, device_id={"sp": s - 1}, device_id_type=pl.DeviceIdType.MESH
        )

    @pl.when(s < spread - 1)
    def _():
        pl.semaphore_signal(
            barrier, inc=1, device_id={"sp": s + 1}, device_id_type=pl.DeviceIdType.MESH
        )

    pl.semaphore_wait(barrier, seqs - 1 + (s + spread - 1) // spread + 1 - (s + 1) // spread)

    load_tok.wait()
    part = pl.ds(pl.multiple_of(core * half, half), half)
    beside = remote(tok.at[0], tok.at[1], tok_send.at[0], tok_recv.at[0], dp=peer(1))
    over = [
        remote(
            tok.at[held, part], tok.at[2 + i, part], tok_send.at[1 + i], tok_recv.at[1 + i],
            dp=(1 - chip) * 2 + core,
        )
        for i, held in enumerate((core, 1 - core))
    ]
    onward = [
        remote(
            tok.at[2 + i, part], tok.at[2 + i, part], tok_send.at[3 + i], tok_recv.at[3 + i],
            dp=peer(1),
        )
        for i in range(2)
    ]
    beside.start()

    @pl.when(core == 0)
    def _():
        over[0].start()

    def unit(vectors):
        vectors = vectors.astype(jnp.bfloat16).astype(jnp.float32)
        return head_norm(vectors, QK_FLOOR).astype(jnp.bfloat16)

    here = pl.ds(pl.multiple_of(s * rows, rows), rows)

    def kv_copy(slot, block):
        piece = kv.at[slot, :, pl.ds(pl.multiple_of(block * rows, rows), rows)]
        return remote(
            piece, piece, kv_send_sem.at[slot, block], kv_recv_sem.at[slot, block],
            sp=(s + 1) % spread,
        )

    def gate_chain(block):
        piece = gates.at[block]
        return remote(
            piece, piece, chain_send_sem.at[block], chain_recv_sem.at[block], sp=(s + 1) % spread
        )

    def project_kv(slot):
        pair = jnp.dot(tok[slot], kvw[...], preferred_element_type=jnp.float32)
        kv[slot, 0, here] = unit(pair[:, :head_dim])
        kv[slot, 1, here] = pair[:, head_dim:].astype(jnp.bfloat16)

        @pl.when(s < spread - 1)
        def _():
            kv_copy(slot, s).start()

    def project_q(slot):
        queries = jnp.dot(tok[slot], qw[...], preferred_element_type=jnp.float32)
        for h in range(heads):
            q_unit[slot, pl.ds(h * rows, rows)] = unit(
                queries[:, h * head_dim : (h + 1) * head_dim]
            )

    load_k.wait()
    load_v.wait()
    project_kv(0)
    beside.wait_recv()

    @pl.when(core == 1)
    def _():
        over[0].start()

    over[1].start()

    forget_input = (
        lax.dot_general(
            fw_in[...], tok[0], (((1,), (1,)), ((), ())), preferred_element_type=jnp.float32
        )
        + off_in[...]
    ).astype(jnp.bfloat16)
    count = bias_in.shape[1]
    square = (count, count)
    diagonal = lax.broadcasted_iota(jnp.int32, square, 0) == lax.broadcasted_iota(
        jnp.int32, square, 1
    )
    bias = jnp.sum(
        jnp.where(diagonal, jnp.broadcast_to(bias_in[...], square), 0.0), axis=1, keepdims=True
    )
    gate_arg = forget_input.astype(jnp.float32) + bias
    log_gate = jnp.minimum(gate_arg, 0.0) - jnp.log1p(jnp.exp(-jnp.abs(gate_arg)))
    before = lax.broadcasted_iota(jnp.int32, (rows, rows), 0)
    after = lax.broadcasted_iota(jnp.int32, (rows, rows), 1)
    running = jnp.dot(
        log_gate,
        (before <= after).astype(jnp.float32),
        preferred_element_type=jnp.float32,
        precision=lax.Precision.HIGHEST,
    )
    gate_send[...] = jnp.zeros_like(gate_send)
    for c in range(seqs):
        gate_send[c, :heads, :] = running[c * heads : (c + 1) * heads]
    gates[s, 0] = gate_send[d]
    gate_out = [
        remote(
            gate_send.at[peer(step)], gates.at[s, seen_as(step)], gate_send_sem.at[step],
            gate_recv_sem.at[seen_as(step)], dp=peer(step),
        )
        for step in range(1, seqs)
    ]
    for copy in gate_out:
        copy.start()

    project_kv(1)
    load_q.wait()
    project_q(0)

    def relay(first, stop, units, with_gates=False):
        @pl.when(s < spread - 1)
        def _():
            def one(k, carry):
                block = s - k
                if with_gates:
                    gate_chain(block).wait_recv()
                    gate_chain(block).start()
                for slot in units:
                    kv_copy(slot, block).wait_recv()
                    kv_copy(slot, block).start()
                return carry

            lax.fori_loop(first, stop, one, 0)

    mine = pl.ds(pl.multiple_of(d * cols, cols), cols)

    def out_copy(slot, arrival):
        return remote(
            sent.at[slot], result.at[:, mine], out_send_sem.at[slot], out_recv_sem.at[arrival],
            dp=peer(slot),
        )

    def attend(slot, blocks):
        span = blocks * rows
        prefix = jnp.zeros((gates.shape[2], 1), jnp.float32)
        totals = []
        for b in range(blocks):
            local_sum = gates[b, slot]
            totals.append(local_sum + prefix)
            prefix = prefix + local_sum[:, rows - 1 :]
        by_row = jnp.transpose(totals[-1])
        by_key = jnp.concatenate(totals, axis=1)
        row = lax.broadcasted_iota(jnp.int32, (rows, span), 0) + (span - rows)
        column = lax.broadcasted_iota(jnp.int32, (rows, span), 1)
        allowed = column <= row
        keys = kv[slot, 0, :span]
        values = kv[slot, 1, :span]
        for h in range(heads):
            scores = lax.dot_general(
                q_unit[slot, pl.ds(h * rows, rows)],
                keys,
                (((1,), (1,)), ((), ())),
                preferred_element_type=jnp.float32,
            )
            factor = gain_in[0, d * heads + h] * head_dim ** (-0.5)
            scores = scores * factor + by_row[:, h : h + 1] - by_key[h : h + 1, :]
            scores = jnp.where(allowed, scores, NEG)
            exponent = jnp.exp(scores - jnp.max(scores, axis=-1, keepdims=True))
            scale = 1.0 / jnp.sum(exponent, axis=-1, keepdims=True)
            weights = (exponent * scale).astype(jnp.bfloat16)
            mixed = jnp.dot(weights, values, preferred_element_type=jnp.float32)
            gain = norm_in[:, pl.ds(pl.multiple_of(d * cols + h * head_dim, head_dim), head_dim)]
            sent[slot, :, h * head_dim : (h + 1) * head_dim] = (
                head_norm(mixed, OUT_FLOOR) * gain
            ).astype(jnp.bfloat16)

    def finish(first, stop, places):
        def each(slot, carry):
            for known in range(first, stop):
                if spread - 1 in places:

                    @pl.when(jnp.logical_and(last, slot == known))
                    def _():
                        def arrive(k, inner):
                            if known == 2:
                                gate_chain(s - k).wait_recv()
                            kv_copy(known, s - k).wait_recv()
                            return inner

                        lax.fori_loop(1, s + 1, arrive, 0)

            for k in places:

                @pl.when(s == k)
                def _():
                    attend(slot, k + 1)

                    @pl.when(slot > 0)
                    def _():
                        out_copy(slot, seen_as(slot)).start()

                    @pl.when(slot == 0)
                    def _():
                        result[:, mine] = sent[0]

            return carry

        lax.fori_loop(first, stop, each, 0)

    some = (s + spread - 1) // spread
    relay(1, 1 + some, [0, 1])
    over[0].wait_recv()
    onward[0].start()
    for step in range(1, seqs):
        pltpu.make_async_copy(
            gates.at[s, step], gates.at[s, step], gate_recv_sem.at[step]
        ).wait()

    @pl.when(s < spread - 1)
    def _():
        gate_chain(s).start()

    onward[0].wait_recv()
    project_kv(2)
    project_q(1)
    relay(2, s + 1, [0, 1])
    relay(1, s + 1, [2], True)
    over[1].wait_recv()
    onward[1].start()
    project_q(2)
    onward[1].wait_recv()
    project_kv(3)
    others = list(range(spread - 1))
    everywhere = list(range(spread))
    relay(1, 1 + some, [3])
    finish(2, 3, everywhere)
    project_q(3)
    relay(2, s + 1, [3])
    finish(0, 2, [spread - 1])
    finish(3, seqs, everywhere)
    finish(0, 2, others)

    def flush(slot, carry):
        out_copy(slot, slot).wait_recv()
        return carry

    lax.fori_loop(1, seqs, flush, 0)
    store = pltpu.make_async_copy(result, out_ref, store_sem.at[0])
    store.start()
    for slot in range(1, seqs):
        out_copy(slot, slot).wait_send()
    for copy in over + [beside] + onward + gate_out:
        copy.wait_send()

    @pl.when(s < spread - 1)
    def _():
        def drain(block, carry):
            gate_chain(block).wait_send()
            for slot in range(seqs):
                kv_copy(slot, block).wait_send()
            return carry

        lax.fori_loop(0, s + 1, drain, 0)

    store.wait()


def fused(
    tokens,
    forget_offset,
    q_weight,
    k_weight,
    v_weight,
    forget_weight,
    forget_bias,
    score_gain,
    out_gain,
):
    rows, width = tokens.shape[1:]
    head_count = forget_bias.shape[0]
    head_dim = out_gain.shape[0] // head_count
    seqs = lax.axis_size("dp")
    spread = lax.axis_size("sp")
    cols = q_weight.shape[1]
    heads = cols // head_dim
    padded = -(-heads // 8) * 8
    anywhere = pl.BlockSpec(memory_space=pl.ANY)
    vmem = pl.BlockSpec(memory_space=pltpu.VMEM)
    dma = pltpu.SemaphoreType.DMA
    out = pl.pallas_call(
        fused_kernel,
        out_shape=jax.ShapeDtypeStruct((rows, seqs * cols), jnp.bfloat16),
        in_specs=[anywhere, vmem, anywhere, anywhere, anywhere, vmem, vmem,
                  pl.BlockSpec(memory_space=pltpu.SMEM), vmem],
        out_specs=anywhere,
        scratch_shapes=[
            pltpu.VMEM((seqs, rows, width), jnp.bfloat16),
            pltpu.VMEM((width, cols), jnp.bfloat16),
            pltpu.VMEM((width, 2 * head_dim), jnp.bfloat16),
            pltpu.VMEM((seqs, heads * rows, head_dim), jnp.bfloat16),
            pltpu.VMEM((seqs, 2, spread * rows, head_dim), jnp.bfloat16),
            pltpu.VMEM((seqs, padded, rows), jnp.float32),
            pltpu.VMEM((spread, seqs, padded, rows), jnp.float32),
            pltpu.VMEM((seqs, rows, cols), jnp.bfloat16),
            pltpu.VMEM((rows, seqs * cols), jnp.bfloat16),
            dma((4,)),
            dma((5,)),
            dma((5,)),
            dma((seqs,)),
            dma((seqs,)),
            dma((seqs, spread)),
            dma((seqs, spread)),
            dma((spread,)),
            dma((spread,)),
            dma((seqs,)),
            dma((seqs,)),
            dma((1,)),
        ],
        compiler_params=pltpu.CompilerParams(collective_id=0, has_side_effects=True),
    )(
        tokens[0],
        forget_offset,
        q_weight,
        k_weight,
        v_weight,
        forget_weight.T,
        forget_bias[None, :],
        score_gain[None, :],
        out_gain[None, :],
    )
    return out[None]


def local(*args):
    tokens, k_weight, forget_bias, out_gain = args[0], args[3], args[6], args[8]
    head_dim = out_gain.shape[0] // forget_bias.shape[0]
    if lax.axis_size("dp") == 4 and k_weight.shape[1] == head_dim and tokens.shape[0] == 1:
        return fused(*args)
    if k_weight.shape[1] % head_dim == 0 and tokens.shape[0] == 1:
        return heads_on_dp(*args)
    return heads_on_sp(*args)


def solution(mesh):
    in_specs = (
        P(("grp", "dp"), "sp", None),
        P(("grp", "dp"), "sp"),
        P(None, "dp"),
        P(None, "dp"),
        P(None, "dp"),
        P(),
        P(),
        P(),
        P(),
    )
    out_specs = P(("grp", "dp"), "sp", None)
    return jax.shard_map(local, mesh=mesh, in_specs=in_specs, out_specs=out_specs, check_vma=False)
```

```python
import jax
import jax.numpy as jnp
from jax import lax
from jax.experimental import pallas as pl
from jax.experimental.pallas import tpu as pltpu
from jax.sharding import PartitionSpec as P

NEG = -1e30
QK_FLOOR = 0.1
OUT_FLOOR = 0.001


def head_norm(vectors, floor):
    return vectors * lax.rsqrt(jnp.mean(vectors * vectors, axis=-1, keepdims=True) + floor)


def heads_on_sp(
    tokens,
    forget_offset,
    q_weight,
    k_weight,
    v_weight,
    forget_weight,
    forget_bias,
    score_gain,
    out_gain,
):
    own_rows = tokens[0]
    tok_count = own_rows.shape[0]
    head_count = forget_bias.shape[0]
    head_dim = out_gain.shape[0] // head_count
    kv_heads = k_weight.shape[1] * lax.axis_size("dp") // head_dim
    spread = lax.axis_size("sp")
    local_heads = head_count // spread
    local_kv = max(1, kv_heads // spread)
    group_size = local_heads // local_kv
    everyone = lax.all_gather(tokens, "dp", axis=0, tiled=True)
    seq_count = everyone.shape[0]
    flat_rows = everyone.reshape(seq_count * tok_count, everyone.shape[2])
    query_cols = (
        jnp.dot(flat_rows, q_weight, preferred_element_type=jnp.float32)
        .astype(jnp.bfloat16)
        .reshape(seq_count, tok_count, -1)
    )
    key_cols = (
        jnp.dot(flat_rows, k_weight, preferred_element_type=jnp.float32)
        .astype(jnp.bfloat16)
        .reshape(seq_count, tok_count, -1)
    )
    value_cols = (
        jnp.dot(flat_rows, v_weight, preferred_element_type=jnp.float32)
        .astype(jnp.bfloat16)
        .reshape(seq_count, tok_count, -1)
    )
    query_mine, key_mine, value_mine = (
        lax.all_to_all(query_cols, "dp", split_axis=0, concat_axis=2, tiled=True),
        lax.all_to_all(key_cols, "dp", split_axis=0, concat_axis=2, tiled=True),
        lax.all_to_all(value_cols, "dp", split_axis=0, concat_axis=2, tiled=True),
    )
    queries = query_mine[0]
    keys_proj = key_mine[0]
    values_proj = value_mine[0]
    forget_input = (
        jnp.dot(own_rows, forget_weight, preferred_element_type=jnp.float32)
        + forget_offset[0][:, None]
    ).astype(jnp.bfloat16)
    query_send = queries.reshape(tok_count, spread, local_heads, head_dim)
    forget_send = forget_input.reshape(tok_count, spread, local_heads)
    if kv_heads >= spread:
        key_send = keys_proj.reshape(tok_count, spread, local_kv, head_dim)
        value_send = values_proj.reshape(tok_count, spread, local_kv, head_dim)
    else:
        copies = spread // kv_heads
        key_send = jnp.broadcast_to(
            keys_proj.reshape(tok_count, kv_heads, 1, head_dim),
            (tok_count, kv_heads, copies, head_dim),
        ).reshape(tok_count, spread, 1, head_dim)
        value_send = jnp.broadcast_to(
            values_proj.reshape(tok_count, kv_heads, 1, head_dim),
            (tok_count, kv_heads, copies, head_dim),
        ).reshape(tok_count, spread, 1, head_dim)
    query_head, forget_head, key_head, value_head = (
        lax.all_to_all(query_send, "sp", split_axis=1, concat_axis=0, tiled=True),
        lax.all_to_all(forget_send, "sp", split_axis=1, concat_axis=0, tiled=True),
        lax.all_to_all(key_send, "sp", split_axis=1, concat_axis=0, tiled=True),
        lax.all_to_all(value_send, "sp", split_axis=1, concat_axis=0, tiled=True),
    )
    length = query_head.shape[0]
    first_head = lax.axis_index("sp") * local_heads
    bias_local = lax.dynamic_slice_in_dim(forget_bias, first_head, local_heads, 0)
    gain_local = lax.dynamic_slice_in_dim(score_gain, first_head, local_heads, 0)
    norm_local = lax.dynamic_slice_in_dim(
        out_gain, first_head * head_dim, local_heads * head_dim, 0
    )
    log_gate = jax.nn.log_sigmoid(
        forget_head.reshape(length, local_heads).astype(jnp.float32) + bias_local[None, :]
    )
    cumulative = jnp.cumsum(log_gate, axis=0).reshape(length, local_kv, group_size)
    query_unit = head_norm(query_head.astype(jnp.float32), QK_FLOOR).astype(jnp.bfloat16)
    key_unit = head_norm(
        key_head.reshape(length, local_kv, head_dim).astype(jnp.float32), QK_FLOOR
    ).astype(jnp.bfloat16)
    value_heads = value_head.reshape(length, local_kv, head_dim)
    factor = (gain_local * head_dim ** (-0.5)).reshape(local_kv, group_size)
    out_gains = norm_local.reshape(local_kv, group_size, head_dim)
    key_totals = jnp.transpose(cumulative, (1, 2, 0))
    span_rows = 512
    positions = jnp.arange(length, dtype=jnp.int32)

    def attend_block(block_index):
        first = block_index * span_rows
        query_block = lax.dynamic_slice_in_dim(query_unit, first, span_rows, 0)
        query_totals = lax.dynamic_slice_in_dim(cumulative, first, span_rows, 0)
        scores = jnp.einsum(
            "qkgd,skd->kgqs", query_block, key_unit, preferred_element_type=jnp.float32
        )
        scores = (
            scores * factor[:, :, None, None]
            + jnp.transpose(query_totals, (1, 2, 0))[..., None]
            - key_totals[:, :, None, :]
        )
        allowed = positions[None, :] <= (first + jnp.arange(span_rows, dtype=jnp.int32))[:, None]
        scores = jnp.where(allowed[None, None], scores, NEG)
        row_peak = jnp.max(scores, axis=-1, keepdims=True)
        exponent = jnp.exp(scores - row_peak)
        weights = (exponent / jnp.sum(exponent, axis=-1, keepdims=True)).astype(jnp.bfloat16)
        mixed = jnp.einsum(
            "kgqs,skd->qkgd", weights, value_heads, preferred_element_type=jnp.float32
        )
        return (head_norm(mixed, OUT_FLOOR) * out_gains).astype(jnp.bfloat16)

    outputs = lax.map(attend_block, jnp.arange(length // span_rows, dtype=jnp.int32))
    outputs = outputs.reshape(length, local_heads, head_dim)
    back_rows = lax.all_to_all(outputs, "sp", split_axis=0, concat_axis=1, tiled=True)
    return back_rows.reshape(1, tok_count, head_count * head_dim)


def heads_on_dp(
    tokens,
    forget_offset,
    q_weight,
    k_weight,
    v_weight,
    forget_weight,
    forget_bias,
    score_gain,
    out_gain,
):
    tok_count = tokens.shape[1]
    head_count = forget_bias.shape[0]
    head_dim = out_gain.shape[0] // head_count
    seq_count = lax.axis_size("dp")
    kv = k_weight.shape[1] // head_dim
    heads = q_weight.shape[1] // head_dim
    group = heads // kv
    everyone = lax.all_gather(tokens, "dp", axis=0, tiled=True)
    offsets = lax.all_gather(forget_offset, "dp", axis=0, tiled=True)
    flat = everyone.reshape(seq_count * tok_count, -1)
    first = lax.axis_index("dp") * heads

    def mine(array):
        return lax.dynamic_slice_in_dim(array, first, heads, array.ndim - 1)

    def project(weight):
        return jnp.dot(flat, weight, preferred_element_type=jnp.float32).astype(jnp.bfloat16)

    key_unit = head_norm(
        project(k_weight).astype(jnp.float32).reshape(seq_count, tok_count, kv, head_dim), QK_FLOOR
    ).astype(jnp.bfloat16)
    values = project(v_weight).reshape(seq_count, tok_count, kv, head_dim)
    pair = lax.all_gather(jnp.stack([key_unit, values]), "sp", axis=2, tiled=True)
    forget_input = (
        jnp.dot(flat, mine(forget_weight), preferred_element_type=jnp.float32)
        + offsets.reshape(-1)[:, None]
    ).astype(jnp.bfloat16)
    log_gate = jax.nn.log_sigmoid(forget_input.astype(jnp.float32) + mine(forget_bias)[None, :])
    gates = lax.all_gather(
        log_gate.reshape(seq_count, tok_count, heads), "sp", axis=1, tiled=True
    )
    cumulative = jnp.cumsum(gates, axis=1)
    length = gates.shape[1]
    start = lax.axis_index("sp") * tok_count
    own = lax.dynamic_slice_in_dim(cumulative, start, tok_count, 1)
    query_unit = head_norm(
        project(q_weight).astype(jnp.float32).reshape(seq_count, tok_count, kv, group, head_dim),
        QK_FLOOR,
    ).astype(jnp.bfloat16)
    factor = (mine(score_gain) * head_dim ** (-0.5)).reshape(kv, group)
    scores = jnp.einsum(
        "bqkgd,bskd->bkgqs", query_unit, pair[0], preferred_element_type=jnp.float32
    )
    by_head = jnp.transpose(own.reshape(seq_count, tok_count, kv, group), (0, 2, 3, 1))
    by_key = jnp.transpose(cumulative.reshape(seq_count, length, kv, group), (0, 2, 3, 1))
    scores = (
        scores * factor[None, :, :, None, None] + by_head[..., None] - by_key[..., None, :]
    )
    allowed = jnp.arange(length)[None, :] <= (start + jnp.arange(tok_count))[:, None]
    scores = jnp.where(allowed, scores, NEG)
    exponent = jnp.exp(scores - jnp.max(scores, axis=-1, keepdims=True))
    weights = (exponent / jnp.sum(exponent, axis=-1, keepdims=True)).astype(jnp.bfloat16)
    mixed = jnp.einsum(
        "bkgqs,bskd->bqkgd", weights, pair[1], preferred_element_type=jnp.float32
    )
    gains = lax.dynamic_slice_in_dim(out_gain, first * head_dim, heads * head_dim, 0)
    outputs = (head_norm(mixed, OUT_FLOOR) * gains.reshape(kv, group, head_dim)).astype(
        jnp.bfloat16
    )
    outputs = outputs.reshape(seq_count, tok_count, heads * head_dim)
    return lax.all_to_all(outputs, "dp", split_axis=0, concat_axis=2, tiled=True)


def fused_kernel(
    tok_in,
    off_in,
    qw_in,
    kw_in,
    vw_in,
    fw_in,
    bias_in,
    gain_in,
    norm_in,
    out_ref,
    tok,
    qw,
    kvw,
    q_unit,
    kv,
    gate_send,
    gates,
    sent,
    result,
    load_sem,
    tok_send,
    tok_recv,
    gate_send_sem,
    gate_recv_sem,
    kv_send_sem,
    kv_recv_sem,
    chain_send_sem,
    chain_recv_sem,
    out_send_sem,
    out_recv_sem,
    store_sem,
):
    d = lax.axis_index("dp")
    s = lax.axis_index("sp")
    spread = lax.axis_size("sp")
    rows, width = tok_in.shape
    half = rows // 2
    cols = qw_in.shape[1]
    head_dim = kw_in.shape[1]
    heads = cols // head_dim
    seqs = tok.shape[0]
    chip, core = d // 2, d % 2
    last = s == spread - 1

    def peer(step):
        across = step // 2
        own_chip = (1 - across) * ((core + step % 2) % 2)
        return ((chip + across) % 2) * 2 + across * (step % 2) + own_chip

    def seen_as(step):
        return (step // 2) * (2 + core) + (1 - step // 2) * step

    def remote(src, dst, send, recv, **target):
        return pltpu.make_async_remote_copy(
            src_ref=src,
            dst_ref=dst,
            send_sem=send,
            recv_sem=recv,
            device_id=target,
            device_id_type=pl.DeviceIdType.MESH,
        )

    load_tok = pltpu.make_async_copy(tok_in, tok.at[0], load_sem.at[0])
    load_k = pltpu.make_async_copy(kw_in, kvw.at[:, pl.ds(0, head_dim)], load_sem.at[1])
    load_v = pltpu.make_async_copy(vw_in, kvw.at[:, pl.ds(head_dim, head_dim)], load_sem.at[2])
    load_q = pltpu.make_async_copy(qw_in, qw, load_sem.at[3])
    load_tok.start()
    load_k.start()
    load_v.start()
    load_q.start()

    barrier = pltpu.get_barrier_semaphore()
    for step in range(1, seqs):
        pl.semaphore_signal(
            barrier, inc=1, device_id={"dp": peer(step)}, device_id_type=pl.DeviceIdType.MESH
        )

    @pl.when(s > 0)
    def _():
        pl.semaphore_signal(
            barrier, inc=1, device_id={"sp": s - 1}, device_id_type=pl.DeviceIdType.MESH
        )

    @pl.when(s < spread - 1)
    def _():
        pl.semaphore_signal(
            barrier, inc=1, device_id={"sp": s + 1}, device_id_type=pl.DeviceIdType.MESH
        )

    @pl.when(s > 1)
    def _():
        pl.semaphore_signal(
            barrier, inc=1, device_id={"sp": s - 2}, device_id_type=pl.DeviceIdType.MESH
        )

    @pl.when(s < spread - 2)
    def _():
        pl.semaphore_signal(
            barrier, inc=1, device_id={"sp": s + 2}, device_id_type=pl.DeviceIdType.MESH
        )

    below = (s + spread - 1) // spread + (s + spread - 2) // spread
    above = 2 - (s + 1) // spread - (s + 2) // spread
    pl.semaphore_wait(barrier, seqs - 1 + below + above)

    load_tok.wait()
    part = pl.ds(pl.multiple_of(core * half, half), half)
    beside = remote(tok.at[0], tok.at[1], tok_send.at[0], tok_recv.at[0], dp=peer(1))
    over = [
        remote(
            tok.at[held, part], tok.at[2 + i, part], tok_send.at[1 + i], tok_recv.at[1 + i],
            dp=(1 - chip) * 2 + core,
        )
        for i, held in enumerate((core, 1 - core))
    ]
    onward = [
        remote(
            tok.at[2 + i, part], tok.at[2 + i, part], tok_send.at[3 + i], tok_recv.at[3 + i],
            dp=peer(1),
        )
        for i in range(2)
    ]
    beside.start()

    @pl.when(core == 0)
    def _():
        over[0].start()

    def unit(vectors):
        vectors = vectors.astype(jnp.bfloat16).astype(jnp.float32)
        return head_norm(vectors, QK_FLOOR).astype(jnp.bfloat16)

    here = pl.ds(pl.multiple_of(s * rows, rows), rows)

    def kv_copy(slot, block, hop=1):
        piece = kv.at[slot, :, pl.ds(pl.multiple_of(block * rows, rows), rows)]
        return remote(
            piece, piece, kv_send_sem.at[slot, hop - 1, block], kv_recv_sem.at[slot, block],
            sp=(s + hop) % spread,
        )

    def gate_chain(block):
        piece = gates.at[block]
        return remote(
            piece, piece, chain_send_sem.at[block], chain_recv_sem.at[block], sp=(s + 1) % spread
        )

    def project_kv(slot):
        pair = jnp.dot(tok[slot], kvw[...], preferred_element_type=jnp.float32)
        kv[slot, 0, here] = unit(pair[:, :head_dim])
        kv[slot, 1, here] = pair[:, head_dim:].astype(jnp.bfloat16)

        @pl.when(s < spread - 2)
        def _():
            kv_copy(slot, s, 2).start()

        @pl.when(s < spread - 1)
        def _():
            kv_copy(slot, s).start()

    def project_q(slot):
        queries = jnp.dot(tok[slot], qw[...], preferred_element_type=jnp.float32)
        for h in range(heads):
            q_unit[slot, pl.ds(h * rows, rows)] = unit(
                queries[:, h * head_dim : (h + 1) * head_dim]
            )

    load_k.wait()
    load_v.wait()
    project_kv(0)
    beside.wait_recv()

    @pl.when(core == 1)
    def _():
        over[0].start()

    over[1].start()

    forget_input = (
        lax.dot_general(
            fw_in[...], tok[0], (((1,), (1,)), ((), ())), preferred_element_type=jnp.float32
        )
        + off_in[...]
    ).astype(jnp.bfloat16)
    count = bias_in.shape[1]
    square = (count, count)
    diagonal = lax.broadcasted_iota(jnp.int32, square, 0) == lax.broadcasted_iota(
        jnp.int32, square, 1
    )
    bias = jnp.sum(
        jnp.where(diagonal, jnp.broadcast_to(bias_in[...], square), 0.0), axis=1, keepdims=True
    )
    gate_arg = forget_input.astype(jnp.float32) + bias
    log_gate = jnp.minimum(gate_arg, 0.0) - jnp.log1p(jnp.exp(-jnp.abs(gate_arg)))
    before = lax.broadcasted_iota(jnp.int32, (rows, rows), 0)
    after = lax.broadcasted_iota(jnp.int32, (rows, rows), 1)
    running = jnp.dot(
        log_gate,
        (before <= after).astype(jnp.float32),
        preferred_element_type=jnp.float32,
        precision=lax.Precision.HIGHEST,
    )
    gate_send[...] = jnp.zeros_like(gate_send)
    for c in range(seqs):
        gate_send[c, :heads, :] = running[c * heads : (c + 1) * heads]
    gates[s, 0] = gate_send[d]
    gate_out = [
        remote(
            gate_send.at[peer(step)], gates.at[s, seen_as(step)], gate_send_sem.at[step],
            gate_recv_sem.at[seen_as(step)], dp=peer(step),
        )
        for step in range(1, seqs)
    ]
    for copy in gate_out:
        copy.start()

    project_kv(1)
    load_q.wait()
    project_q(0)

    def relay(first, stop, units, with_gates=False):
        @pl.when(s < spread - 1)
        def _():
            def one(k, carry):
                block = s - k
                if with_gates:
                    gate_chain(block).wait_recv()
                    gate_chain(block).start()
                for slot in units:
                    kv_copy(slot, block).wait_recv()
                    kv_copy(slot, block).start()
                return carry

            lax.fori_loop(first, stop, one, 0)

    mine = pl.ds(pl.multiple_of(d * cols, cols), cols)

    def out_copy(slot, arrival):
        return remote(
            sent.at[slot], result.at[:, mine], out_send_sem.at[slot], out_recv_sem.at[arrival],
            dp=peer(slot),
        )

    def attend(slot, blocks):
        span = blocks * rows
        prefix = jnp.zeros((gates.shape[2], 1), jnp.float32)
        totals = []
        for b in range(blocks):
            local_sum = gates[b, slot]
            totals.append(local_sum + prefix)
            prefix = prefix + local_sum[:, rows - 1 :]
        by_row = jnp.transpose(totals[-1])
        by_key = jnp.concatenate(totals, axis=1)
        row = lax.broadcasted_iota(jnp.int32, (rows, span), 0) + (span - rows)
        column = lax.broadcasted_iota(jnp.int32, (rows, span), 1)
        allowed = column <= row
        keys = kv[slot, 0, :span]
        values = kv[slot, 1, :span]
        for h in range(heads):
            scores = lax.dot_general(
                q_unit[slot, pl.ds(h * rows, rows)],
                keys,
                (((1,), (1,)), ((), ())),
                preferred_element_type=jnp.float32,
            )
            factor = gain_in[0, d * heads + h] * head_dim ** (-0.5)
            scores = scores * factor + by_row[:, h : h + 1] - by_key[h : h + 1, :]
            scores = jnp.where(allowed, scores, NEG)
            exponent = jnp.exp(scores - jnp.max(scores, axis=-1, keepdims=True))
            scale = 1.0 / jnp.sum(exponent, axis=-1, keepdims=True)
            weights = (exponent * scale).astype(jnp.bfloat16)
            mixed = jnp.dot(weights, values, preferred_element_type=jnp.float32)
            gain = norm_in[:, pl.ds(pl.multiple_of(d * cols + h * head_dim, head_dim), head_dim)]
            sent[slot, :, h * head_dim : (h + 1) * head_dim] = (
                head_norm(mixed, OUT_FLOOR) * gain
            ).astype(jnp.bfloat16)

    some = (s + spread - 1) // spread

    def member(places):
        if len(places) == spread:
            return s >= 0
        return last if places[0] == spread - 1 else s < spread - 1

    def finish(first, stop, places):
        def each(slot, carry):
            for known in range(first, stop):
                @pl.when(jnp.logical_and(member(places), slot == known))
                def _():
                    def arrive(k, inner):
                        if known == 2:

                            @pl.when(last)
                            def _():
                                gate_chain(s - k).wait_recv()

                        kv_copy(known, s - k).wait_recv()
                        return inner

                    lax.fori_loop(1, 1 + some + (s + 1) // spread * (s - some), arrive, 0)

            for k in places:

                @pl.when(s == k)
                def _():
                    attend(slot, k + 1)

                    @pl.when(slot > 0)
                    def _():
                        out_copy(slot, seen_as(slot)).start()

                    @pl.when(slot == 0)
                    def _():
                        result[:, mine] = sent[0]

            return carry

        lax.fori_loop(first, stop, each, 0)

    some = (s + spread - 1) // spread
    over[0].wait_recv()
    onward[0].start()
    for step in range(1, seqs):
        pltpu.make_async_copy(
            gates.at[s, step], gates.at[s, step], gate_recv_sem.at[step]
        ).wait()

    @pl.when(s < spread - 1)
    def _():
        gate_chain(s).start()

    onward[0].wait_recv()
    project_kv(2)
    project_q(1)
    relay(2, s + 1, [0, 1])
    relay(1, s + 1, [], True)
    relay(2, s + 1, [2])
    over[1].wait_recv()
    onward[1].start()
    project_q(2)
    onward[1].wait_recv()
    project_kv(3)
    others = list(range(spread - 1))
    everywhere = list(range(spread))
    finish(2, 3, everywhere)
    project_q(3)
    relay(2, s + 1, [3])
    finish(0, 2, [spread - 1])
    finish(3, seqs, everywhere)
    finish(0, 2, others)

    def flush(slot, carry):
        out_copy(slot, slot).wait_recv()
        return carry

    lax.fori_loop(1, seqs, flush, 0)
    store = pltpu.make_async_copy(result, out_ref, store_sem.at[0])
    store.start()
    for slot in range(1, seqs):
        out_copy(slot, slot).wait_send()
    for copy in over + [beside] + onward + gate_out:
        copy.wait_send()

    @pl.when(s < spread - 1)
    def _():
        def drain_gates(block, carry):
            gate_chain(block).wait_send()
            return carry

        def drain(block, carry):
            for slot in range(seqs):
                kv_copy(slot, block).wait_send()
            return carry

        lax.fori_loop(0, s + 1, drain_gates, 0)
        lax.fori_loop(0, s - 1, drain, 0)
        drain(s, 0)

    @pl.when(s < spread - 2)
    def _():
        for slot in range(seqs):
            kv_copy(slot, s, 2).wait_send()

    store.wait()


def fused(
    tokens,
    forget_offset,
    q_weight,
    k_weight,
    v_weight,
    forget_weight,
    forget_bias,
    score_gain,
    out_gain,
):
    rows, width = tokens.shape[1:]
    head_count = forget_bias.shape[0]
    head_dim = out_gain.shape[0] // head_count
    seqs = lax.axis_size("dp")
    spread = lax.axis_size("sp")
    cols = q_weight.shape[1]
    heads = cols // head_dim
    padded = -(-heads // 8) * 8
    anywhere = pl.BlockSpec(memory_space=pl.ANY)
    vmem = pl.BlockSpec(memory_space=pltpu.VMEM)
    dma = pltpu.SemaphoreType.DMA
    out = pl.pallas_call(
        fused_kernel,
        out_shape=jax.ShapeDtypeStruct((rows, seqs * cols), jnp.bfloat16),
        in_specs=[anywhere, vmem, anywhere, anywhere, anywhere, vmem, vmem,
                  pl.BlockSpec(memory_space=pltpu.SMEM), vmem],
        out_specs=anywhere,
        scratch_shapes=[
            pltpu.VMEM((seqs, rows, width), jnp.bfloat16),
            pltpu.VMEM((width, cols), jnp.bfloat16),
            pltpu.VMEM((width, 2 * head_dim), jnp.bfloat16),
            pltpu.VMEM((seqs, heads * rows, head_dim), jnp.bfloat16),
            pltpu.VMEM((seqs, 2, spread * rows, head_dim), jnp.bfloat16),
            pltpu.VMEM((seqs, padded, rows), jnp.float32),
            pltpu.VMEM((spread, seqs, padded, rows), jnp.float32),
            pltpu.VMEM((seqs, rows, cols), jnp.bfloat16),
            pltpu.VMEM((rows, seqs * cols), jnp.bfloat16),
            dma((4,)),
            dma((5,)),
            dma((5,)),
            dma((seqs,)),
            dma((seqs,)),
            dma((seqs, 2, spread)),
            dma((seqs, spread)),
            dma((spread,)),
            dma((spread,)),
            dma((seqs,)),
            dma((seqs,)),
            dma((1,)),
        ],
        compiler_params=pltpu.CompilerParams(collective_id=0, has_side_effects=True),
    )(
        tokens[0],
        forget_offset,
        q_weight,
        k_weight,
        v_weight,
        forget_weight.T,
        forget_bias[None, :],
        score_gain[None, :],
        out_gain[None, :],
    )
    return out[None]


def local(*args):
    tokens, k_weight, forget_bias, out_gain = args[0], args[3], args[6], args[8]
    head_dim = out_gain.shape[0] // forget_bias.shape[0]
    if lax.axis_size("dp") == 4 and k_weight.shape[1] == head_dim and tokens.shape[0] == 1:
        return fused(*args)
    if k_weight.shape[1] % head_dim == 0 and tokens.shape[0] == 1:
        return heads_on_dp(*args)
    return heads_on_sp(*args)


def solution(mesh):
    in_specs = (
        P(("grp", "dp"), "sp", None),
        P(("grp", "dp"), "sp"),
        P(None, "dp"),
        P(None, "dp"),
        P(None, "dp"),
        P(),
        P(),
        P(),
        P(),
    )
    out_specs = P(("grp", "dp"), "sp", None)
    return jax.shard_map(local, mesh=mesh, in_specs=in_specs, out_specs=out_specs, check_vma=False)
```

```python
import jax
import jax.numpy as jnp
from jax import lax
from jax.experimental import pallas as pl
from jax.experimental.pallas import tpu as pltpu
from jax.sharding import PartitionSpec as P

NEG = -1e30
QK_FLOOR = 0.1
OUT_FLOOR = 0.001


def head_norm(vectors, floor):
    return vectors * lax.rsqrt(jnp.mean(vectors * vectors, axis=-1, keepdims=True) + floor)


def heads_on_sp(
    tokens,
    forget_offset,
    q_weight,
    k_weight,
    v_weight,
    forget_weight,
    forget_bias,
    score_gain,
    out_gain,
):
    own_rows = tokens[0]
    tok_count = own_rows.shape[0]
    head_count = forget_bias.shape[0]
    head_dim = out_gain.shape[0] // head_count
    kv_heads = k_weight.shape[1] * lax.axis_size("dp") // head_dim
    spread = lax.axis_size("sp")
    local_heads = head_count // spread
    local_kv = max(1, kv_heads // spread)
    group_size = local_heads // local_kv
    everyone = lax.all_gather(tokens, "dp", axis=0, tiled=True)
    seq_count = everyone.shape[0]
    flat_rows = everyone.reshape(seq_count * tok_count, everyone.shape[2])
    query_cols = (
        jnp.dot(flat_rows, q_weight, preferred_element_type=jnp.float32)
        .astype(jnp.bfloat16)
        .reshape(seq_count, tok_count, -1)
    )
    key_cols = (
        jnp.dot(flat_rows, k_weight, preferred_element_type=jnp.float32)
        .astype(jnp.bfloat16)
        .reshape(seq_count, tok_count, -1)
    )
    value_cols = (
        jnp.dot(flat_rows, v_weight, preferred_element_type=jnp.float32)
        .astype(jnp.bfloat16)
        .reshape(seq_count, tok_count, -1)
    )
    query_mine, key_mine, value_mine = (
        lax.all_to_all(query_cols, "dp", split_axis=0, concat_axis=2, tiled=True),
        lax.all_to_all(key_cols, "dp", split_axis=0, concat_axis=2, tiled=True),
        lax.all_to_all(value_cols, "dp", split_axis=0, concat_axis=2, tiled=True),
    )
    queries = query_mine[0]
    keys_proj = key_mine[0]
    values_proj = value_mine[0]
    forget_input = (
        jnp.dot(own_rows, forget_weight, preferred_element_type=jnp.float32)
        + forget_offset[0][:, None]
    ).astype(jnp.bfloat16)
    query_send = queries.reshape(tok_count, spread, local_heads, head_dim)
    forget_send = forget_input.reshape(tok_count, spread, local_heads)
    if kv_heads >= spread:
        key_send = keys_proj.reshape(tok_count, spread, local_kv, head_dim)
        value_send = values_proj.reshape(tok_count, spread, local_kv, head_dim)
    else:
        copies = spread // kv_heads
        key_send = jnp.broadcast_to(
            keys_proj.reshape(tok_count, kv_heads, 1, head_dim),
            (tok_count, kv_heads, copies, head_dim),
        ).reshape(tok_count, spread, 1, head_dim)
        value_send = jnp.broadcast_to(
            values_proj.reshape(tok_count, kv_heads, 1, head_dim),
            (tok_count, kv_heads, copies, head_dim),
        ).reshape(tok_count, spread, 1, head_dim)
    query_head, forget_head, key_head, value_head = (
        lax.all_to_all(query_send, "sp", split_axis=1, concat_axis=0, tiled=True),
        lax.all_to_all(forget_send, "sp", split_axis=1, concat_axis=0, tiled=True),
        lax.all_to_all(key_send, "sp", split_axis=1, concat_axis=0, tiled=True),
        lax.all_to_all(value_send, "sp", split_axis=1, concat_axis=0, tiled=True),
    )
    length = query_head.shape[0]
    first_head = lax.axis_index("sp") * local_heads
    bias_local = lax.dynamic_slice_in_dim(forget_bias, first_head, local_heads, 0)
    gain_local = lax.dynamic_slice_in_dim(score_gain, first_head, local_heads, 0)
    norm_local = lax.dynamic_slice_in_dim(
        out_gain, first_head * head_dim, local_heads * head_dim, 0
    )
    log_gate = jax.nn.log_sigmoid(
        forget_head.reshape(length, local_heads).astype(jnp.float32) + bias_local[None, :]
    )
    cumulative = jnp.cumsum(log_gate, axis=0).reshape(length, local_kv, group_size)
    query_unit = head_norm(query_head.astype(jnp.float32), QK_FLOOR).astype(jnp.bfloat16)
    key_unit = head_norm(
        key_head.reshape(length, local_kv, head_dim).astype(jnp.float32), QK_FLOOR
    ).astype(jnp.bfloat16)
    value_heads = value_head.reshape(length, local_kv, head_dim)
    factor = (gain_local * head_dim ** (-0.5)).reshape(local_kv, group_size)
    out_gains = norm_local.reshape(local_kv, group_size, head_dim)
    key_totals = jnp.transpose(cumulative, (1, 2, 0))
    span_rows = 512
    positions = jnp.arange(length, dtype=jnp.int32)

    def attend_block(block_index):
        first = block_index * span_rows
        query_block = lax.dynamic_slice_in_dim(query_unit, first, span_rows, 0)
        query_totals = lax.dynamic_slice_in_dim(cumulative, first, span_rows, 0)
        scores = jnp.einsum(
            "qkgd,skd->kgqs", query_block, key_unit, preferred_element_type=jnp.float32
        )
        scores = (
            scores * factor[:, :, None, None]
            + jnp.transpose(query_totals, (1, 2, 0))[..., None]
            - key_totals[:, :, None, :]
        )
        allowed = positions[None, :] <= (first + jnp.arange(span_rows, dtype=jnp.int32))[:, None]
        scores = jnp.where(allowed[None, None], scores, NEG)
        row_peak = jnp.max(scores, axis=-1, keepdims=True)
        exponent = jnp.exp(scores - row_peak)
        weights = (exponent / jnp.sum(exponent, axis=-1, keepdims=True)).astype(jnp.bfloat16)
        mixed = jnp.einsum(
            "kgqs,skd->qkgd", weights, value_heads, preferred_element_type=jnp.float32
        )
        return (head_norm(mixed, OUT_FLOOR) * out_gains).astype(jnp.bfloat16)

    outputs = lax.map(attend_block, jnp.arange(length // span_rows, dtype=jnp.int32))
    outputs = outputs.reshape(length, local_heads, head_dim)
    back_rows = lax.all_to_all(outputs, "sp", split_axis=0, concat_axis=1, tiled=True)
    return back_rows.reshape(1, tok_count, head_count * head_dim)


def heads_on_dp(
    tokens,
    forget_offset,
    q_weight,
    k_weight,
    v_weight,
    forget_weight,
    forget_bias,
    score_gain,
    out_gain,
):
    tok_count = tokens.shape[1]
    head_count = forget_bias.shape[0]
    head_dim = out_gain.shape[0] // head_count
    seq_count = lax.axis_size("dp")
    kv = k_weight.shape[1] // head_dim
    heads = q_weight.shape[1] // head_dim
    group = heads // kv
    everyone = lax.all_gather(tokens, "dp", axis=0, tiled=True)
    offsets = lax.all_gather(forget_offset, "dp", axis=0, tiled=True)
    flat = everyone.reshape(seq_count * tok_count, -1)
    first = lax.axis_index("dp") * heads

    def mine(array):
        return lax.dynamic_slice_in_dim(array, first, heads, array.ndim - 1)

    def project(weight):
        return jnp.dot(flat, weight, preferred_element_type=jnp.float32).astype(jnp.bfloat16)

    key_unit = head_norm(
        project(k_weight).astype(jnp.float32).reshape(seq_count, tok_count, kv, head_dim), QK_FLOOR
    ).astype(jnp.bfloat16)
    values = project(v_weight).reshape(seq_count, tok_count, kv, head_dim)
    pair = lax.all_gather(jnp.stack([key_unit, values]), "sp", axis=2, tiled=True)
    forget_input = (
        jnp.dot(flat, mine(forget_weight), preferred_element_type=jnp.float32)
        + offsets.reshape(-1)[:, None]
    ).astype(jnp.bfloat16)
    log_gate = jax.nn.log_sigmoid(forget_input.astype(jnp.float32) + mine(forget_bias)[None, :])
    gates = lax.all_gather(
        log_gate.reshape(seq_count, tok_count, heads), "sp", axis=1, tiled=True
    )
    cumulative = jnp.cumsum(gates, axis=1)
    length = gates.shape[1]
    start = lax.axis_index("sp") * tok_count
    own = lax.dynamic_slice_in_dim(cumulative, start, tok_count, 1)
    query_unit = head_norm(
        project(q_weight).astype(jnp.float32).reshape(seq_count, tok_count, kv, group, head_dim),
        QK_FLOOR,
    ).astype(jnp.bfloat16)
    factor = (mine(score_gain) * head_dim ** (-0.5)).reshape(kv, group)
    scores = jnp.einsum(
        "bqkgd,bskd->bkgqs", query_unit, pair[0], preferred_element_type=jnp.float32
    )
    by_head = jnp.transpose(own.reshape(seq_count, tok_count, kv, group), (0, 2, 3, 1))
    by_key = jnp.transpose(cumulative.reshape(seq_count, length, kv, group), (0, 2, 3, 1))
    scores = (
        scores * factor[None, :, :, None, None] + by_head[..., None] - by_key[..., None, :]
    )
    allowed = jnp.arange(length)[None, :] <= (start + jnp.arange(tok_count))[:, None]
    scores = jnp.where(allowed, scores, NEG)
    exponent = jnp.exp(scores - jnp.max(scores, axis=-1, keepdims=True))
    weights = (exponent / jnp.sum(exponent, axis=-1, keepdims=True)).astype(jnp.bfloat16)
    mixed = jnp.einsum(
        "bkgqs,bskd->bqkgd", weights, pair[1], preferred_element_type=jnp.float32
    )
    gains = lax.dynamic_slice_in_dim(out_gain, first * head_dim, heads * head_dim, 0)
    outputs = (head_norm(mixed, OUT_FLOOR) * gains.reshape(kv, group, head_dim)).astype(
        jnp.bfloat16
    )
    outputs = outputs.reshape(seq_count, tok_count, heads * head_dim)
    return lax.all_to_all(outputs, "dp", split_axis=0, concat_axis=2, tiled=True)


def fused_kernel(
    tok_in,
    off_in,
    qw_in,
    kw_in,
    vw_in,
    fw_in,
    bias_in,
    gain_in,
    norm_in,
    out_ref,
    tok,
    qw,
    kvw,
    q_unit,
    kv,
    gate_send,
    gates,
    sent,
    result,
    load_sem,
    tok_send,
    tok_recv,
    gate_send_sem,
    gate_recv_sem,
    kv_send_sem,
    kv_recv_sem,
    chain_send_sem,
    chain_recv_sem,
    out_send_sem,
    out_recv_sem,
    store_sem,
):
    d = lax.axis_index("dp")
    s = lax.axis_index("sp")
    spread = lax.axis_size("sp")
    rows, width = tok_in.shape
    half = rows // 2
    cols = qw_in.shape[1]
    head_dim = kw_in.shape[1]
    heads = cols // head_dim
    seqs = tok.shape[0]
    chip, core = d // 2, d % 2
    last = s == spread - 1

    def peer(step):
        across = step // 2
        own_chip = (1 - across) * ((core + step % 2) % 2)
        return ((chip + across) % 2) * 2 + across * (step % 2) + own_chip

    def seen_as(step):
        return (step // 2) * (2 + core) + (1 - step // 2) * step

    def remote(src, dst, send, recv, **target):
        return pltpu.make_async_remote_copy(
            src_ref=src,
            dst_ref=dst,
            send_sem=send,
            recv_sem=recv,
            device_id=target,
            device_id_type=pl.DeviceIdType.MESH,
        )

    load_tok = pltpu.make_async_copy(tok_in, tok.at[0], load_sem.at[0])
    load_k = pltpu.make_async_copy(kw_in, kvw.at[:, pl.ds(0, head_dim)], load_sem.at[1])
    load_v = pltpu.make_async_copy(vw_in, kvw.at[:, pl.ds(head_dim, head_dim)], load_sem.at[2])
    load_q = pltpu.make_async_copy(qw_in, qw, load_sem.at[3])
    load_tok.start()
    load_k.start()
    load_v.start()
    load_q.start()

    barrier = pltpu.get_barrier_semaphore()
    for step in range(1, seqs):
        pl.semaphore_signal(
            barrier, inc=1, device_id={"dp": peer(step)}, device_id_type=pl.DeviceIdType.MESH
        )

    @pl.when(s > 0)
    def _():
        pl.semaphore_signal(
            barrier, inc=1, device_id={"sp": s - 1}, device_id_type=pl.DeviceIdType.MESH
        )

    @pl.when(s < spread - 1)
    def _():
        pl.semaphore_signal(
            barrier, inc=1, device_id={"sp": s + 1}, device_id_type=pl.DeviceIdType.MESH
        )

    pl.semaphore_wait(barrier, seqs - 1 + (s + spread - 1) // spread + 1 - (s + 1) // spread)

    load_tok.wait()
    part = pl.ds(pl.multiple_of(core * half, half), half)
    beside = remote(tok.at[0], tok.at[1], tok_send.at[0], tok_recv.at[0], dp=peer(1))
    over = [
        remote(
            tok.at[held, part], tok.at[2 + i, part], tok_send.at[1 + i], tok_recv.at[1 + i],
            dp=(1 - chip) * 2 + core,
        )
        for i, held in enumerate((core, 1 - core))
    ]
    onward = [
        remote(
            tok.at[2 + i, part], tok.at[2 + i, part], tok_send.at[3 + i], tok_recv.at[3 + i],
            dp=peer(1),
        )
        for i in range(2)
    ]
    beside.start()

    @pl.when(core == 0)
    def _():
        over[0].start()

    def unit(vectors):
        vectors = vectors.astype(jnp.bfloat16).astype(jnp.float32)
        return head_norm(vectors, QK_FLOOR).astype(jnp.bfloat16)

    here = pl.ds(pl.multiple_of(s * rows, rows), rows)

    def kv_copy(slot, block):
        piece = kv.at[slot, :, pl.ds(pl.multiple_of(block * rows, rows), rows)]
        return remote(
            piece, piece, kv_send_sem.at[slot, block], kv_recv_sem.at[slot, block],
            sp=(s + 1) % spread,
        )

    def gate_chain(block):
        piece = gates.at[block]
        return remote(
            piece, piece, chain_send_sem.at[block], chain_recv_sem.at[block], sp=(s + 1) % spread
        )

    def project_kv(slot):
        pair = jnp.dot(tok[slot], kvw[...], preferred_element_type=jnp.float32)
        kv[slot, 0, here] = unit(pair[:, :head_dim])
        kv[slot, 1, here] = pair[:, head_dim:].astype(jnp.bfloat16)

        @pl.when(s < spread - 1)
        def _():
            kv_copy(slot, s).start()

    def project_q(slot):
        queries = jnp.dot(tok[slot], qw[...], preferred_element_type=jnp.float32)
        for h in range(heads):
            q_unit[slot, pl.ds(h * rows, rows)] = unit(
                queries[:, h * head_dim : (h + 1) * head_dim]
            )

    load_k.wait()
    load_v.wait()
    project_kv(0)
    beside.wait_recv()

    @pl.when(core == 1)
    def _():
        over[0].start()

    over[1].start()

    forget_input = (
        lax.dot_general(
            fw_in[...], tok[0], (((1,), (1,)), ((), ())), preferred_element_type=jnp.float32
        )
        + off_in[...]
    ).astype(jnp.bfloat16)
    count = bias_in.shape[1]
    square = (count, count)
    diagonal = lax.broadcasted_iota(jnp.int32, square, 0) == lax.broadcasted_iota(
        jnp.int32, square, 1
    )
    bias = jnp.sum(
        jnp.where(diagonal, jnp.broadcast_to(bias_in[...], square), 0.0), axis=1, keepdims=True
    )
    gate_arg = forget_input.astype(jnp.float32) + bias
    log_gate = jnp.minimum(gate_arg, 0.0) - jnp.log1p(jnp.exp(-jnp.abs(gate_arg)))
    before = lax.broadcasted_iota(jnp.int32, (rows, rows), 0)
    after = lax.broadcasted_iota(jnp.int32, (rows, rows), 1)
    running = jnp.dot(
        log_gate,
        (before <= after).astype(jnp.float32),
        preferred_element_type=jnp.float32,
        precision=lax.Precision.HIGHEST,
    )
    gate_send[...] = jnp.zeros_like(gate_send)
    for c in range(seqs):
        gate_send[c, :heads, :] = running[c * heads : (c + 1) * heads]
    gates[s, 0] = gate_send[d]
    gate_out = [
        remote(
            gate_send.at[peer(step)], gates.at[s, seen_as(step)], gate_send_sem.at[step],
            gate_recv_sem.at[seen_as(step)], dp=peer(step),
        )
        for step in range(1, seqs)
    ]
    for copy in gate_out:
        copy.start()

    project_kv(1)
    load_q.wait()
    project_q(0)

    def relay(first, stop, units, with_gates=False):
        @pl.when(s < spread - 1)
        def _():
            def one(k, carry):
                block = s - k
                if with_gates:
                    gate_chain(block).wait_recv()
                    gate_chain(block).start()
                for slot in units:
                    kv_copy(slot, block).wait_recv()
                    kv_copy(slot, block).start()
                return carry

            lax.fori_loop(first, stop, one, 0)

    mine = pl.ds(pl.multiple_of(d * cols, cols), cols)

    def out_copy(slot, arrival):
        return remote(
            sent.at[slot], result.at[:, mine], out_send_sem.at[slot], out_recv_sem.at[arrival],
            dp=peer(slot),
        )

    def attend(slot, blocks):
        span = blocks * rows
        prefix = jnp.zeros((gates.shape[2], 1), jnp.float32)
        totals = []
        for b in range(blocks):
            local_sum = gates[b, slot]
            totals.append(local_sum + prefix)
            prefix = prefix + local_sum[:, rows - 1 :]
        by_row = jnp.transpose(totals[-1])
        by_key = jnp.concatenate(totals, axis=1)
        row = lax.broadcasted_iota(jnp.int32, (rows, span), 0) + (span - rows)
        column = lax.broadcasted_iota(jnp.int32, (rows, span), 1)
        allowed = column <= row
        keys = kv[slot, 0, :span]
        values = kv[slot, 1, :span]
        for h in range(heads):
            scores = lax.dot_general(
                q_unit[slot, pl.ds(h * rows, rows)],
                keys,
                (((1,), (1,)), ((), ())),
                preferred_element_type=jnp.float32,
            )
            factor = gain_in[0, d * heads + h] * head_dim ** (-0.5)
            scores = scores * factor + by_row[:, h : h + 1] - by_key[h : h + 1, :]
            scores = jnp.where(allowed, scores, NEG)
            exponent = jnp.exp(scores - jnp.max(scores, axis=-1, keepdims=True))
            scale = 1.0 / jnp.sum(exponent, axis=-1, keepdims=True)
            weights = (exponent * scale).astype(jnp.bfloat16)
            mixed = jnp.dot(weights, values, preferred_element_type=jnp.float32)
            gain = norm_in[:, pl.ds(pl.multiple_of(d * cols + h * head_dim, head_dim), head_dim)]
            sent[slot, :, h * head_dim : (h + 1) * head_dim] = (
                head_norm(mixed, OUT_FLOOR) * gain
            ).astype(jnp.bfloat16)

    def finish(first, stop, places):
        def each(slot, carry):
            for known in range(first, stop):
                if spread - 1 in places:

                    @pl.when(jnp.logical_and(last, slot == known))
                    def _():
                        def arrive(k, inner):
                            if known == 2:
                                gate_chain(s - k).wait_recv()
                            kv_copy(known, s - k).wait_recv()
                            return inner

                        lax.fori_loop(1, s + 1, arrive, 0)

            for k in places:

                @pl.when(s == k)
                def _():
                    attend(slot, k + 1)

                    @pl.when(slot > 0)
                    def _():
                        out_copy(slot, seen_as(slot)).start()

                    @pl.when(slot == 0)
                    def _():
                        result[:, mine] = sent[0]

            return carry

        lax.fori_loop(first, stop, each, 0)

    some = (s + spread - 1) // spread
    relay(1, 1 + some, [0, 1])
    over[0].wait_recv()
    onward[0].start()
    for step in range(1, seqs):
        pltpu.make_async_copy(
            gates.at[s, step], gates.at[s, step], gate_recv_sem.at[step]
        ).wait()

    @pl.when(s < spread - 1)
    def _():
        gate_chain(s).start()

    onward[0].wait_recv()
    project_kv(2)
    project_q(1)
    relay(2, s + 1, [0, 1])
    relay(1, s + 1, [2], True)
    over[1].wait_recv()
    onward[1].start()
    project_q(2)
    onward[1].wait_recv()
    project_kv(3)
    others = list(range(spread - 1))
    everywhere = list(range(spread))
    relay(1, 1 + some, [3])
    project_q(3)
    relay(2, s + 1, [3])
    finish(2, 3, everywhere)
    finish(0, 2, [spread - 1])
    finish(3, seqs, everywhere)
    finish(0, 2, others)

    def flush(slot, carry):
        out_copy(slot, slot).wait_recv()
        return carry

    lax.fori_loop(1, seqs, flush, 0)
    store = pltpu.make_async_copy(result, out_ref, store_sem.at[0])
    store.start()
    for slot in range(1, seqs):
        out_copy(slot, slot).wait_send()
    for copy in over + [beside] + onward + gate_out:
        copy.wait_send()

    @pl.when(s < spread - 1)
    def _():
        def drain(block, carry):
            gate_chain(block).wait_send()
            for slot in range(seqs):
                kv_copy(slot, block).wait_send()
            return carry

        lax.fori_loop(0, s + 1, drain, 0)

    store.wait()


def fused(
    tokens,
    forget_offset,
    q_weight,
    k_weight,
    v_weight,
    forget_weight,
    forget_bias,
    score_gain,
    out_gain,
):
    rows, width = tokens.shape[1:]
    head_count = forget_bias.shape[0]
    head_dim = out_gain.shape[0] // head_count
    seqs = lax.axis_size("dp")
    spread = lax.axis_size("sp")
    cols = q_weight.shape[1]
    heads = cols // head_dim
    padded = -(-heads // 8) * 8
    anywhere = pl.BlockSpec(memory_space=pl.ANY)
    vmem = pl.BlockSpec(memory_space=pltpu.VMEM)
    dma = pltpu.SemaphoreType.DMA
    out = pl.pallas_call(
        fused_kernel,
        out_shape=jax.ShapeDtypeStruct((rows, seqs * cols), jnp.bfloat16),
        in_specs=[anywhere, vmem, anywhere, anywhere, anywhere, vmem, vmem,
                  pl.BlockSpec(memory_space=pltpu.SMEM), vmem],
        out_specs=anywhere,
        scratch_shapes=[
            pltpu.VMEM((seqs, rows, width), jnp.bfloat16),
            pltpu.VMEM((width, cols), jnp.bfloat16),
            pltpu.VMEM((width, 2 * head_dim), jnp.bfloat16),
            pltpu.VMEM((seqs, heads * rows, head_dim), jnp.bfloat16),
            pltpu.VMEM((seqs, 2, spread * rows, head_dim), jnp.bfloat16),
            pltpu.VMEM((seqs, padded, rows), jnp.float32),
            pltpu.VMEM((spread, seqs, padded, rows), jnp.float32),
            pltpu.VMEM((seqs, rows, cols), jnp.bfloat16),
            pltpu.VMEM((rows, seqs * cols), jnp.bfloat16),
            dma((4,)),
            dma((5,)),
            dma((5,)),
            dma((seqs,)),
            dma((seqs,)),
            dma((seqs, spread)),
            dma((seqs, spread)),
            dma((spread,)),
            dma((spread,)),
            dma((seqs,)),
            dma((seqs,)),
            dma((1,)),
        ],
        compiler_params=pltpu.CompilerParams(collective_id=0, has_side_effects=True),
    )(
        tokens[0],
        forget_offset,
        q_weight,
        k_weight,
        v_weight,
        forget_weight.T,
        forget_bias[None, :],
        score_gain[None, :],
        out_gain[None, :],
    )
    return out[None]


def local(*args):
    tokens, k_weight, forget_bias, out_gain = args[0], args[3], args[6], args[8]
    head_dim = out_gain.shape[0] // forget_bias.shape[0]
    if lax.axis_size("dp") == 4 and k_weight.shape[1] == head_dim and tokens.shape[0] == 1:
        return fused(*args)
    if k_weight.shape[1] % head_dim == 0 and tokens.shape[0] == 1:
        return heads_on_dp(*args)
    return heads_on_sp(*args)


def solution(mesh):
    in_specs = (
        P(("grp", "dp"), "sp", None),
        P(("grp", "dp"), "sp"),
        P(None, "dp"),
        P(None, "dp"),
        P(None, "dp"),
        P(),
        P(),
        P(),
        P(),
    )
    out_specs = P(("grp", "dp"), "sp", None)
    return jax.shard_map(local, mesh=mesh, in_specs=in_specs, out_specs=out_specs, check_vma=False)
```
